128 devices in a mesh: fs: 16 (over z, x), tp: 8 (over y, core).
Axes of the slice: x: 4, y: 4, z: 4, core: 2. Of those that a mesh axis runs over, the one named last changes fastest.
Arguments:
- tokens: bfloat16 [16384, 2048], P(('fs', 'tp')), may hold values from -130 to 130
- pool_weight: bfloat16 [4, 512, 512], P(None, 'fs'), may hold values from -0.25 to 0.25
- pool_scale: float32 [2048], replicated, may hold values from 0.5 to 1.5
- gain_mix: float32 [2048], replicated, may hold values from 0.1 to 1.9
- gain_mlp: float32 [2048], replicated, may hold values from 0.1 to 1.9
- w_up: bfloat16 [8192, 2048], P('tp', 'fs'), may hold values from -0.125 to 0.125
- w_down: bfloat16 [8192, 2048], P('tp', 'fs'), may hold values from -0.0625 to 0.0625
- gain_out: float32 [2048], P('tp'), may hold values from 0.1 to 1.9
Outputs:
- result: bfloat16 [16384, 2048], P('fs', 'tp')
The draws below stay inside these ranges and needn't reach their ends.
All inputs are finite; a program needn't handle non-finite values.
Results may differ from the reference program's by a relative error of at most 0.013.
Values may be sent and summed in bfloat16 or wider, within the bound.
A program may use at most 64 MiB of HBM per device.

```python
import math
import jax
import jax.numpy as jnp
from jax import lax

D = 2048
FF = 8192
GROUP = 512
SEQ_LEN = 1024
TOKENS = 16384
N_TP = 8


def draw_tokens(key, part):
    key_row, key_col, key_base = jax.random.split(jax.random.fold_in(key, 11), 3)
    column = jnp.arange(D, dtype=jnp.float32) / D
    row_scale = jnp.exp(jax.random.uniform(key_row, (TOKENS, 1), jnp.float32, math.log(0.5), math.log(5.0)))
    col_scale = jnp.exp(jax.random.uniform(key_col, (1, D), jnp.float32, math.log(0.4), math.log(2.5)))
    base = jnp.clip(jax.random.normal(key_base, (TOKENS, D), jnp.float32), -4.0, 4.0)
    trend = 3.0 ** (0.5 * column)
    return (base * row_scale * col_scale * trend[None, :]).astype(jnp.bfloat16)


def steps_of(key, dims, shards, least, largest):
    factor_of, own = 1.0, jax.random.fold_in(key, 6)
    for dim, shards_of in shards:
        heights = jnp.exp(jax.random.uniform(jax.random.fold_in(own, dim), (shards_of,), jnp.float32, least / len(shards), largest / len(shards)))
        factor_of = factor_of * jnp.repeat(heights, dims[dim] // shards_of).reshape([-1 if axis == dim else 1 for axis in range(len(dims))])
    return factor_of


def centred(stream_key, extent, spread, most, cuts=(), kind=jnp.bfloat16):
    level = steps_of(stream_key, extent, cuts, -0.22, 0.18) if cuts else 1.0
    drawn = jax.random.normal(stream_key, extent, jnp.float32) * spread * level
    return jnp.minimum(jnp.maximum(drawn, -most), most).astype(kind)


def setup_inputs(seed: int = 0) -> dict:
    arg_keys = jax.random.split(jax.random.key(seed), 9)
    tokens = draw_tokens(jax.random.fold_in(arg_keys[8], 71), 0)
    pool_weight = centred(arg_keys[1], (4, GROUP, GROUP), GROUP ** -0.5, 0.25, ((1, 16),))
    pool_scale = jnp.clip(jax.random.uniform(arg_keys[2], (D,), jnp.float32, 0.5, 1.5), 0.5, 1.5)
    gain_mix = jnp.clip(1.0 + 0.18 * jax.random.normal(arg_keys[3], (D,), jnp.float32), 0.1, 1.9)
    gain_mlp = jnp.clip(1.0 + 0.18 * jax.random.normal(arg_keys[4], (D,), jnp.float32), 0.1, 1.9)
    w_up = centred(arg_keys[5], (FF, D), D ** -0.5, 0.125, ((0, 8), (1, 16)))
    w_down = centred(arg_keys[6], (FF, D), FF ** -0.5, 0.0625, ((0, 8), (1, 16)))
    gain_out = jnp.clip(1.0 + 0.18 * jax.random.normal(arg_keys[7], (D,), jnp.float32), 0.1, 1.9)
    return dict(tokens=tokens, pool_weight=pool_weight, pool_scale=pool_scale, gain_mix=gain_mix, gain_mlp=gain_mlp, w_up=w_up, w_down=w_down, gain_out=gain_out)


EPS = 1e-06
WINDOWS = (2, 4, 8, 16)

def rms_scale(values, gain):
    return values * lax.rsqrt(lax.optimization_barrier(jnp.mean(values * values, axis=-1, keepdims=True)) + EPS) * gain

def window_mean(values, reach):
    cumulative = jnp.concatenate([jnp.zeros_like(values[:, :1]), jnp.cumsum(values, axis=1)], axis=1)
    position = jnp.arange(SEQ_LEN, dtype=jnp.int32)
    lower = jnp.clip(position - reach // 2, 0, SEQ_LEN).astype(jnp.int32)
    upper = jnp.clip(position + reach // 2, 0, SEQ_LEN).astype(jnp.int32)
    sums = jnp.take(cumulative, upper, axis=1) - jnp.take(cumulative, lower, axis=1)
    counts = (upper - lower).astype(jnp.float32)[None, :, None]
    return sums / counts

def reference(tokens, pool_weight, pool_scale, gain_mix, gain_mlp, w_up, w_down, gain_out):
    inputs = tokens.astype(jnp.float32)
    normed = rms_scale(inputs, gain_mix).astype(jnp.bfloat16)
    normed_seq = normed.astype(jnp.float32).reshape(-1, SEQ_LEN, D)
    pieces = []
    for index, reach in enumerate(WINDOWS):
        part = normed_seq[..., index * GROUP:(index + 1) * GROUP]
        pooled = (window_mean(part, reach) - part).astype(jnp.bfloat16).reshape(-1, GROUP)
        pieces.append(jnp.dot(pooled, pool_weight[index], preferred_element_type=jnp.float32))
    mixed = jnp.concatenate(pieces, axis=1) * pool_scale
    first_sum = (inputs + mixed).astype(jnp.bfloat16)
    first_f32 = first_sum.astype(jnp.float32)
    inner = rms_scale(first_f32, gain_mlp).astype(jnp.bfloat16)
    block = FF // N_TP

    def add_block(index, total):
        begin = (index * block).astype(jnp.int32)
        up_block = lax.dynamic_slice_in_dim(w_up, begin, block, 0)
        down_block = lax.dynamic_slice_in_dim(w_down, begin, block, 0)
        pre = jnp.dot(inner, up_block.T, preferred_element_type=jnp.float32)
        hidden = jnp.square(jax.nn.relu(pre)).astype(jnp.bfloat16)
        partial_sum = jnp.dot(hidden, down_block, preferred_element_type=jnp.float32).astype(jnp.bfloat16)
        partial_sum = lax.optimization_barrier(partial_sum)
        return total + partial_sum.astype(jnp.float32)
    channel_out = lax.fori_loop(jnp.int32(0), jnp.int32(N_TP), add_block, jnp.zeros((tokens.shape[0], D), jnp.float32))
    second_sum = first_f32 + channel_out
    return rms_scale(second_sum, gain_out).astype(jnp.bfloat16)
```

```python
import functools

import jax
import jax.numpy as jnp
from jax import lax
from jax.experimental import pallas as pl
from jax.experimental.pallas import tpu as pltpu
from jax.sharding import PartitionSpec as P

D = 2048
SEQ = 1024
EPS = 1e-06
F32 = jnp.float32
BF16 = jnp.bfloat16
MESH = pl.DeviceIdType.MESH
CH = 256
NCH = SEQ // CH
HALF = SEQ // 2


def kernel(tok, pw, up, dn, pscale, gmix, gmlp, gout, out,
           tokv, X, NB, R, RT, PB, UB, DB, PL2, G, SQ, SQ2, H, PART, SO, SB, RH, RY, ACC,
           lsem, as_, ar, rs_, rr, ps, pr, us, ur, ds_, dr, xs, xr, gs, gr, ss, sr, ts, tr, cs, cr, ys, yr):
    f = lax.axis_index("fs")
    t = lax.axis_index("tp")
    z, x = f // 4, f % 4
    y, c = t // 2, t % 2

    def fa(d):
        return (1 - c) * (4 * z + (x + d) % 4) + c * (4 * ((z + d) % 4) + x)

    def fb(d):
        return (1 - c) * (4 * ((z + d) % 4) + x) + c * (4 * z + (x + d) % 4)

    pa = (1 - c) * x + c * z
    pb = (1 - c) * z + c * x

    def slot(i, j):
        return 4 * ((pb + j) % 4) + (pa + i) % 4

    def slot_of(g):
        return (1 - c) * g + c * (4 * (g % 4) + g // 4)

    def remote(src, dst, ssem, rsem, fs, tp):
        return pltpu.make_async_remote_copy(
            src_ref=src, dst_ref=dst, send_sem=ssem, recv_sem=rsem,
            device_id={"fs": fs, "tp": tp}, device_id_type=MESH)

    sib = 2 * y + 1 - c
    yp = 2 * ((y + 1) % 4) + c
    ym = 2 * ((y + 3) % 4) + c
    own = slot(0, 0)

    c_tok = pltpu.make_async_copy(tok, tokv, lsem.at[0])
    c_x = pltpu.make_async_copy(
        tok.at[:, pl.ds(pl.multiple_of(256 * t, 256), 256)],
        X.at[pl.ds(pl.multiple_of(128 * t, 128), 128)], lsem.at[1])
    c_u = pltpu.make_async_copy(up, UB.at[own], lsem.at[2])
    c_d = pltpu.make_async_copy(dn, DB.at[own], lsem.at[3])
    c_p = pltpu.make_async_copy(
        pw.at[y, :, pl.ds(pl.multiple_of(256 * c, 256), 256)], PB.at[own], lsem.at[4])
    for cp in (c_tok, c_p, c_u, c_x, c_d):
        cp.start()
    barrier = pltpu.get_barrier_semaphore()
    for e in (1, 2, 3):
        pl.semaphore_signal(barrier, inc=1, device_id={"fs": fa(e), "tp": t}, device_id_type=MESH)
        pl.semaphore_signal(barrier, inc=1, device_id={"fs": fb(e), "tp": t}, device_id_type=MESH)
    for e in range(1, 8):
        pl.semaphore_signal(barrier, inc=1, device_id={"fs": f, "tp": (t + e) % 8}, device_id_type=MESH)
    c_tok.wait()
    c_p.wait()
    c_u.wait()
    pl.semaphore_wait(barrier, 13)

    def a2a(e):
        p = (t + e) % 8
        return remote(tokv.at[:, pl.ds(pl.multiple_of(256 * p, 256), 256)],
                      X.at[pl.ds(pl.multiple_of(128 * t, 128), 128)], as_.at[e - 1], ar.at[e - 1], f, p)

    for e in (4, 3, 5, 2, 6, 1, 7):
        a2a(e).start()

    def p_a(e):
        return remote(PB.at[own], PB.at[own], ps.at[e - 1], pr.at[e - 1], fa(e), t)

    def p_b(e):
        line = PB.at[pl.ds(4 * pb, 4)]
        return remote(line, line, ps.at[2 + e], pr.at[2 + e], fb(e), t)

    for e in (1, 3, 2):
        p_a(e).start()

    hrows = (pl.ds(0, HALF), pl.ds(HALF, HALF))
    offs = (0, 3, 1, 2)

    def w_a0(W, s, r, d):
        ref = W.at[own]
        return remote(ref, ref, s.at[d], r.at[d], fa(1 if d == 0 else 3), t)

    def w_a2(W, s, r, d):
        ref = W.at[slot(3 if d == 0 else 1, 0), hrows[d]]
        return remote(ref, ref, s.at[2 + d], r.at[2 + d], fa(1 if d == 0 else 3), t)

    def w_b(W, s, r, n, d):
        ref = W.at[slot(offs[n], 0)]
        return remote(ref, ref, s.at[4 + 2 * n + d], r.at[4 + 2 * n + d], fb(1 if d == 0 else 3), t)

    def w_b2(W, s, r, n, d):
        ref = W.at[slot(offs[n], 3 if d == 0 else 1), hrows[d]]
        return remote(ref, ref, s.at[12 + 2 * n + d], r.at[12 + 2 * n + d], fb(1 if d == 0 else 3), t)

    def pump_a0(W, s, r):
        for d in (0, 1):
            w_a0(W, s, r, d).start()

    def pump_b(W, s, r, n):
        for d in (0, 1):
            w_b(W, s, r, n, d).start()

    def pump_a1(W, s, r):
        for d in (0, 1):
            w_a0(W, s, r, d).wait_recv()
        for d in (0, 1):
            w_a2(W, s, r, d).start()
        pump_b(W, s, r, 1)
        pump_b(W, s, r, 2)

    def pump_a2(W, s, r):
        for d in (0, 1):
            w_a2(W, s, r, d).wait_recv()
        pump_b(W, s, r, 3)

    def pump_b1(W, s, r, n):
        for d in (0, 1):
            w_b(W, s, r, n, d).wait_recv()
            w_b2(W, s, r, n, d).start()

    def pump_b2(W, s, r, n):
        for d in (0, 1):
            w_b2(W, s, r, n, d).wait_recv()

    U = (UB, us, ur)
    V = (DB, ds_, dr)
    pump_a0(*U)

    ri = lax.broadcasted_iota(jnp.int32, (128, 128), 0)
    ci = lax.broadcasted_iota(jnp.int32, (128, 128), 1)
    eye = (ri == ci).astype(F32)

    def to_lanes(col):
        return jnp.sum(col * eye, axis=0, keepdims=True)

    def to_column(lanes):
        return jnp.sum(lanes * eye, axis=1, keepdims=True)

    v = tokv[...].astype(F32)
    r1 = lax.rsqrt(jnp.sum(v * v, axis=1, keepdims=True) / D + EPS)
    R[t] = jnp.broadcast_to(to_lanes(r1), (8, 128))

    def r_x(e):
        return remote(R.at[t], R.at[t], rs_.at[e - 1], rr.at[e - 1], f, (t + e) % 8)

    for e in range(1, 8):
        r_x(e).start()

    for e in (1, 3, 2):
        p_a(e).wait_recv()
    for e in (1, 3, 2):
        p_b(e).start()
    pump_b(*U, 0)
    pump_a1(*U)

    def row_of(ref):
        return jnp.concatenate([ref[pl.ds(2 * t, 1), :], ref[pl.ds(2 * t + 1, 1), :]], axis=1)

    gm = row_of(gmix)
    NB[pl.ds(0, 16), :] = jnp.zeros((16, 256), BF16)
    NB[pl.ds(16 + SEQ, 16), :] = jnp.zeros((16, 256), BF16)
    c_x.wait()
    c_d.wait()
    for e in range(1, 8):
        a2a(e).wait_recv()
        r_x(e).wait_recv()
    for i in range(8):
        rc = to_column(R[i, 0:1, :])
        xv = X[pl.ds(128 * i, 128), :].astype(F32)
        NB[pl.ds(16 + 128 * i, 128), :] = (xv * rc * gm).astype(BF16)

    reach = 1 + (y >= 1).astype(jnp.int32) + 2 * (y >= 2).astype(jnp.int32) + 4 * (y >= 3).astype(jnp.int32)
    bi = lax.broadcasted_iota(jnp.int32, (128, 160), 0)
    bj = lax.broadcasted_iota(jnp.int32, (128, 160), 1)
    delta = bj - 16 - bi
    band = jnp.where((delta >= -reach) & (delta < reach), 1.0, 0.0).astype(BF16)

    def pl_x(q):
        ref = PL2.at[c, pl.ds(CH * q, CH)]
        return remote(ref, ref, xs.at[q], xr.at[q], f, sib)

    for i in range(8):
        sums = jnp.dot(band, NB[pl.ds(128 * i, 160), :], preferred_element_type=F32)
        pos = 128 * i + lax.broadcasted_iota(jnp.int32, (128, 256), 0)
        count = jnp.minimum(pos + reach, SEQ) - jnp.maximum(pos - reach, 0)
        mine = NB[pl.ds(16 + 128 * i, 128), :].astype(F32)
        PL2[c, pl.ds(128 * i, 128), :] = (sums / count.astype(F32) - mine).astype(BF16)
        if i % 2 == 1:
            pl_x(i // 2).start()

    pump_a2(*U)
    for e in (1, 3, 2):
        p_b(e).wait_recv()

    psc = row_of(pscale)
    gml = row_of(gmlp)

    def g_ref(owner, q):
        return G.at[owner, pl.ds(CH * q, CH)]

    def g_y(q, d):
        return remote(g_ref(t, q), g_ref(t, q), gs.at[2 * q + d], gr.at[2 * q + d], f, yp if d == 0 else ym)

    def g_sib(k, q):
        owner = (t + (0, 6, 2, 4)[k]) % 8
        return remote(g_ref(owner, q), g_ref(owner, q), gs.at[8 + 4 * k + q], gr.at[8 + 4 * k + q], f, sib)

    def g_fwd(q):
        owner = ym if q < 2 else yp
        return remote(g_ref(owner, q), g_ref(owner, q), gs.at[24 + q], gr.at[24 + q], f, yp if q < 2 else ym)

    pk = [jnp.concatenate([PB[slot_of(8 * k + i)] for i in range(8)], axis=0) for k in (0, 1)]
    for q in range(NCH):
        pl_x(q).wait_recv()
        rows = pl.ds(CH * q, CH)
        mixed = (jnp.dot(PL2[0, rows, :], pk[0], preferred_element_type=F32)
                 + jnp.dot(PL2[1, rows, :], pk[1], preferred_element_type=F32)) * psc
        first = (X[rows, :].astype(F32) + mixed).astype(BF16).astype(F32)
        G[t, rows, :] = (first * gml).astype(BF16)
        for d in (0, 1):
            g_y(q, d).start()
        g_sib(0, q).start()
        ACC[0, rows, :] = first[:, :128]
        ACC[1, rows, :] = first[:, 128:]
        sq = jnp.sum(first * first, axis=1, keepdims=True)
        for h in (0, 1):
            SQ[t, pl.ds(2 * q + h, 1), :] = to_lanes(sq[128 * h:128 * h + 128])

    def sq_x(e):
        return remote(SQ.at[t], SQ.at[t], ss.at[e - 1], sr.at[e - 1], f, (t + e) % 8)

    for e in range(1, 8):
        sq_x(e).start()

    def g_pump(q):
        g_y(q, 0).wait_recv()
        if q < 2:
            g_fwd(q).start()
        g_sib(1, q).start()
        g_y(q, 1).wait_recv()
        if q >= 2:
            g_fwd(q).start()
        g_sib(2, q).start()

    def g_pump2(q):
        g_fwd(q).wait_recv()
        g_sib(3, q).start()

    pump_b1(*U, 0)
    g_pump(0)
    pump_b1(*U, 1)
    g_pump(1)
    pump_b1(*U, 2)
    pump_b1(*U, 3)
    pump_a0(*V)
    pump_b(*V, 0)
    g_pump(2)
    g_pump2(0)
    g_pump(3)
    g_pump2(1)
    g_pump2(2)
    for n in range(4):
        pump_b2(*U, n)
    pump_a1(*V)
    g_pump2(3)

    for e in range(1, 8):
        sq_x(e).wait_recv()
    total = SQ[0]
    for i in range(1, 8):
        total = total + SQ[i]
    RT[...] = lax.rsqrt(total / D + EPS)
    for k in range(4):
        for q in range(NCH):
            g_sib(k, q).wait_recv()

    def up_rows(q, carry):
        base = pl.multiple_of(CH * q, CH)
        rows = pl.ds(base, CH)
        rc = jnp.concatenate([to_column(RT[pl.ds(2 * q + h, 1), :]) for h in (0, 1)], axis=0)
        lhs = jnp.concatenate([G[i, rows, :] for i in range(8)], axis=1)

        def cols(h, carry):
            hs = pl.ds(pl.multiple_of(256 * h, 256), 256)
            rhs = jnp.concatenate([UB[slot_of(g), hs, :] for g in range(16)], axis=1)
            pre = lax.dot_general(lhs, rhs, (((1,), (1,)), ((), ())), preferred_element_type=F32)
            act = jnp.maximum(pre * rc, 0.0)
            H[rows, hs] = (act * act).astype(BF16)
            return carry

        return lax.fori_loop(0, 4, cols, carry)

    lax.fori_loop(0, NCH, up_rows, 0)
    pump_a2(*V)
    for n in range(4):
        pump_b1(*V, n)
    for n in range(4):
        pump_b2(*V, n)

    def so(k, d):
        return SO.at[k, d]

    def c_x2(k, d):
        return remote(SO.at[k, d], SB.at[k, d], cs.at[4 * k + d], cr.at[4 * k + d], f, sib)

    def y_half(k, d):
        return remote(SO.at[k, 2, hrows[d]], RH.at[k, d], ys.at[4 * k + d], yr.at[4 * k + d], f, yp if d == 0 else ym)

    def y_full(k, d):
        return remote(SO.at[k, 1 if d == 0 else 3], RY.at[k, d], ys.at[4 * k + 2 + d], yr.at[4 * k + 2 + d], f,
                      yp if d == 0 else ym)

    for k in range(4):
        xk = (x + offs[k]) % 4
        owner = xk // 2 == c
        helper = xk // 2 != c
        half = xk % 2

        def down(q, carry):
            rows = pl.ds(pl.multiple_of(CH * q, CH), CH)
            rhs = jnp.concatenate([DB[slot_of(4 * ((y + d) % 4) + xk)] for d in range(4)], axis=1)
            PART[rows, :] = jnp.dot(H[rows, :], rhs, preferred_element_type=F32)
            return carry

        lax.fori_loop(0, NCH, down, 0)

        @pl.when(helper)
        def _():
            for d in (2, 1, 3, 0):
                SO[k, d] = PART[:, 128 * d:128 * d + 128].astype(BF16)
                c_x2(k, d).start()
            for d in (2, 1, 3, 0):
                c_x2(k, d).wait_send()

        @pl.when(owner)
        def _():
            c_x2(k, 2).wait_recv()
            SO[k, 2] = (PART[:, 256:384] + SB[k, 2].astype(F32)).astype(BF16)
            y_half(k, 0).start()
            y_half(k, 1).start()
            c_x2(k, 1).wait_recv()
            c_x2(k, 3).wait_recv()
            y_half(k, 0).wait_recv()
            SO[k, 1, hrows[0]] = (PART[hrows[0], 128:256] + SB[k, 1, hrows[0]].astype(F32)
                                  + RH[k, 0].astype(F32)).astype(BF16)
            SO[k, 1, hrows[1]] = (PART[hrows[1], 128:256] + SB[k, 1, hrows[1]].astype(F32)).astype(BF16)
            y_full(k, 0).start()
            y_half(k, 1).wait_recv()
            SO[k, 3, hrows[0]] = (PART[hrows[0], 384:512] + SB[k, 3, hrows[0]].astype(F32)).astype(BF16)
            SO[k, 3, hrows[1]] = (PART[hrows[1], 384:512] + SB[k, 3, hrows[1]].astype(F32)
                                  + RH[k, 1].astype(F32)).astype(BF16)
            y_full(k, 1).start()
            c_x2(k, 0).wait_recv()
            ACC[half] = ACC[half] + PART[:, 0:128] + SB[k, 0].astype(F32)

    for k in range(4):
        xk = (x + offs[k]) % 4
        owner = xk // 2 == c
        half = xk % 2

        @pl.when(owner)
        def _():
            y_full(k, 0).wait_recv()
            y_full(k, 1).wait_recv()
            ACC[half] = ACC[half] + RY[k, 0].astype(F32) + RY[k, 1].astype(F32)
            for d in (0, 1):
                y_half(k, d).wait_send()
                y_full(k, d).wait_send()

    for i in range(8):
        rows = pl.ds(128 * i, 128)
        a0, a1 = ACC[0, rows, :], ACC[1, rows, :]
        SQ2[t, pl.ds(i, 1), :] = to_lanes(jnp.sum(a0 * a0 + a1 * a1, axis=1, keepdims=True))

    def t_x(e):
        return remote(SQ2.at[t], SQ2.at[t], ts.at[e - 1], tr.at[e - 1], f, (t + e) % 8)

    for e in range(1, 8):
        t_x(e).start()
    for e in range(1, 8):
        t_x(e).wait_recv()
    total = SQ2[0]
    for i in range(1, 8):
        total = total + SQ2[i]
    rl = lax.rsqrt(total / D + EPS)
    for i in range(8):
        rows = pl.ds(128 * i, 128)
        rc = to_column(rl[i:i + 1, :])
        for h in (0, 1):
            out[rows, 128 * h:128 * h + 128] = (ACC[h, rows, :] * rc * gout[h:h + 1, :]).astype(BF16)

    for e in range(1, 8):
        a2a(e).wait_send()
        r_x(e).wait_send()
        sq_x(e).wait_send()
        t_x(e).wait_send()
    for e in (1, 2, 3):
        p_a(e).wait_send()
        p_b(e).wait_send()
    for W in (U, V):
        for d in (0, 1):
            w_a0(*W, d).wait_send()
            w_a2(*W, d).wait_send()
            for n in range(4):
                w_b(*W, n, d).wait_send()
                w_b2(*W, n, d).wait_send()
    for q in range(NCH):
        pl_x(q).wait_send()
        g_y(q, 0).wait_send()
        g_y(q, 1).wait_send()
        g_fwd(q).wait_send()
        for k in range(4):
            g_sib(k, q).wait_send()


def local(tokens, pool_weight, pool_scale, gain_mix, gain_mlp, w_up, w_down, gain_out):
    dma = pltpu.SemaphoreType.DMA
    hbm = pl.BlockSpec(memory_space=pl.ANY)
    vmem = pl.BlockSpec(memory_space=pltpu.VMEM)
    return pl.pallas_call(
        kernel,
        out_shape=jax.ShapeDtypeStruct((SEQ, 256), BF16),
        in_specs=[hbm] * 4 + [vmem] * 4,
        out_specs=vmem,
        scratch_shapes=[
            pltpu.VMEM((128, D), BF16),
            pltpu.VMEM((SEQ, 256), BF16),
            pltpu.VMEM((SEQ + 32, 256), BF16),
            pltpu.VMEM((8, 8, 128), F32),
            pltpu.VMEM((8, 128), F32),
            pltpu.VMEM((16, 32, 256), BF16),
            pltpu.VMEM((16, 1024, 128), BF16),
            pltpu.VMEM((16, 1024, 128), BF16),
            pltpu.VMEM((2, SEQ, 256), BF16),
            pltpu.VMEM((8, SEQ, 256), BF16),
            pltpu.VMEM((8, 8, 128), F32),
            pltpu.VMEM((8, 8, 128), F32),
            pltpu.VMEM((SEQ, 1024), BF16),
            pltpu.VMEM((SEQ, 512), F32),
            pltpu.VMEM((4, 4, SEQ, 128), BF16),
            pltpu.VMEM((4, 4, SEQ, 128), BF16),
            pltpu.VMEM((4, 2, HALF, 128), BF16),
            pltpu.VMEM((4, 2, SEQ, 128), BF16),
            pltpu.VMEM((2, SEQ, 128), F32),
            dma((5,)),
            dma((7,)), dma((7,)),
            dma((7,)), dma((7,)),
            dma((6,)), dma((6,)),
            dma((20,)), dma((20,)),
            dma((20,)), dma((20,)),
            dma((4,)), dma((4,)),
            dma((28,)), dma((28,)),
            dma((7,)), dma((7,)),
            dma((7,)), dma((7,)),
            dma((16,)), dma((16,)),
            dma((16,)), dma((16,)),
        ],
        compiler_params=pltpu.CompilerParams(
            collective_id=0, has_side_effects=True, vmem_limit_bytes=60 * 1024 * 1024),
        name="mixers",
    )(tokens, pool_weight, w_up, w_down, pool_scale.reshape(16, 128), gain_mix.reshape(16, 128),
      gain_mlp.reshape(16, 128), gain_out.reshape(2, 128))


def solution(mesh):
    placed = (P(("fs", "tp"), None), P(None, "fs", None), P(), P(), P(), P("tp", "fs"), P("tp", "fs"), P("tp"))
    return jax.shard_map(local, mesh=mesh, in_specs=placed, out_specs=P("fs", "tp"), check_vma=False)
```

```python
import functools

import jax
import jax.numpy as jnp
from jax import lax
from jax.experimental import pallas as pl
from jax.experimental.pallas import tpu as pltpu
from jax.sharding import PartitionSpec as P

D = 2048
SEQ = 1024
EPS = 1e-06
F32 = jnp.float32
BF16 = jnp.bfloat16
MESH = pl.DeviceIdType.MESH
CH = 256
NCH = SEQ // CH
HALF = SEQ // 2


class Phases:
    now = None

    def __call__(self, name):
        if self.now is not None:
            self.now.__exit__(None, None, None)
        self.now = jax.named_scope(name) if name else None
        if name:
            self.now.__enter__()


def kernel(tok, pw, up, dn, pscale, gmix, gmlp, gout, out,
           tokv, RL, X, NB, R, RT, PB, UB, DB, PL2, G, SQ, SQ2, H, PART, SO, SB, RH, RY, ACC,
           lsem, as_, ar, rs_, rr, ps, pr, us, ur, ds_, dr, xs, xr, gs, gr, ss, sr, ts, tr, cs, cr, ys, yr):
    ph = Phases()
    f = lax.axis_index("fs")
    t = lax.axis_index("tp")
    z, x = f // 4, f % 4
    y, c = t // 2, t % 2

    def fa(d):
        return (1 - c) * (4 * z + (x + d) % 4) + c * (4 * ((z + d) % 4) + x)

    def fb(d):
        return (1 - c) * (4 * ((z + d) % 4) + x) + c * (4 * z + (x + d) % 4)

    pa = (1 - c) * x + c * z
    pb = (1 - c) * z + c * x

    def slot(i, j):
        return 4 * ((pb + j) % 4) + (pa + i) % 4

    def slot_of(g):
        return (1 - c) * g + c * (4 * (g % 4) + g // 4)

    def remote(src, dst, ssem, rsem, fs, tp):
        return pltpu.make_async_remote_copy(
            src_ref=src, dst_ref=dst, send_sem=ssem, recv_sem=rsem,
            device_id={"fs": fs, "tp": tp}, device_id_type=MESH)

    sib = 2 * y + 1 - c
    yp = 2 * ((y + 1) % 4) + c
    ym = 2 * ((y + 3) % 4) + c
    own = slot(0, 0)

    ph("a_entry")
    c_tok = pltpu.make_async_copy(tok, tokv, lsem.at[0])
    c_x = pltpu.make_async_copy(
        tok.at[:, pl.ds(pl.multiple_of(256 * t, 256), 256)],
        X.at[pl.ds(pl.multiple_of(128 * t, 128), 128)], lsem.at[1])
    c_u = pltpu.make_async_copy(up, UB.at[own], lsem.at[2])
    c_d = pltpu.make_async_copy(dn, DB.at[own], lsem.at[3])
    c_p = pltpu.make_async_copy(
        pw.at[y, :, pl.ds(pl.multiple_of(256 * c, 256), 256)], PB.at[own], lsem.at[4])
    for cp in (c_tok, c_p, c_u, c_x, c_d):
        cp.start()
    barrier = pltpu.get_barrier_semaphore()
    for e in range(1, 8):
        pl.semaphore_signal(barrier, inc=1, device_id={"fs": f, "tp": (t + e) % 8}, device_id_type=MESH)
    for e in (1, 2, 3):
        pl.semaphore_signal(barrier, inc=1, device_id={"fs": fa(e), "tp": t}, device_id_type=MESH)
        pl.semaphore_signal(barrier, inc=1, device_id={"fs": fb(e), "tp": t}, device_id_type=MESH)

    ri = lax.broadcasted_iota(jnp.int32, (128, 128), 0)
    ci = lax.broadcasted_iota(jnp.int32, (128, 128), 1)
    eye = (ri == ci).astype(F32)

    def to_lanes(col):
        return jnp.sum(col * eye, axis=0, keepdims=True)

    def to_column(lanes):
        return jnp.sum(lanes * eye, axis=1, keepdims=True)

    c_tok.wait()
    v = tokv[...].astype(F32)
    r1 = lax.rsqrt(jnp.sum(v * v, axis=1, keepdims=True) / D + EPS)
    R[t] = jnp.broadcast_to(to_lanes(r1), (8, 128))
    c_p.wait()
    c_u.wait()
    c_d.wait()
    pl.semaphore_wait(barrier, 13)

    ph("b_start")
    via = (y + 1 + 2 * c) % 4

    def rows_of(o):
        return pl.ds(pl.multiple_of(128 * o, 128), 128)

    def near(n):
        p = (2 * ((y + (1 if n < 2 else 3)) % 4) + n % 2) if n < 4 else sib
        return remote(tokv.at[:, pl.ds(pl.multiple_of(256 * p, 256), 256)], X.at[rows_of(t)], as_.at[n], ar_of(n), f, p)

    def ar_of(n):
        return ar.at[(2 if n < 2 else 0) + c] if n < 4 else ar.at[4]

    def near_in(n):
        o = (2 * ((y + (1 if n < 2 else 3)) % 4) + n % 2) if n < 4 else sib
        return pltpu.make_async_copy(X.at[rows_of(o)], X.at[rows_of(o)], ar.at[n])

    def relay_out():
        return remote(tokv.at[:, pl.ds(pl.multiple_of(512 * ((y + 2) % 4), 512), 512)], RL,
                      as_.at[5], ar.at[5], f, 2 * via + c)

    def relay_on(k):
        o = 2 * ((y + 3 + 2 * c) % 4) + c
        return remote(RL.at[:, pl.ds(256 * k, 256)], X.at[rows_of(o)], as_.at[6 + k], ar.at[6 + c], f, 2 * via + k)

    def relay_in(k):
        o = 2 * ((y + 2) % 4) + k
        return pltpu.make_async_copy(X.at[rows_of(o)], X.at[rows_of(o)], ar.at[6 + k])

    relay_out().start()
    for n in (0, 2, 1, 3, 4):
        near(n).start()

    def r_x(e):
        return remote(R.at[t], R.at[t], rs_.at[e - 1], rr.at[e - 1], f, (t + e) % 8)

    for e in range(1, 8):
        r_x(e).start()

    def p_a(e):
        return remote(PB.at[own], PB.at[own], ps.at[e - 1], pr.at[e - 1], fa(e), t)

    def p_b(e):
        line = PB.at[pl.ds(4 * pb, 4)]
        return remote(line, line, ps.at[2 + e], pr.at[2 + e], fb(e), t)

    for e in (1, 3, 2):
        p_a(e).start()

    hrows = (pl.ds(0, HALF), pl.ds(HALF, HALF))
    offs = (0, 3, 1, 2)

    def w_a0(W, s, r, d):
        ref = W.at[own]
        return remote(ref, ref, s.at[d], r.at[d], fa(1 if d == 0 else 3), t)

    def w_a2(W, s, r, d):
        ref = W.at[slot(3 if d == 0 else 1, 0), hrows[d]]
        return remote(ref, ref, s.at[2 + d], r.at[2 + d], fa(1 if d == 0 else 3), t)

    def w_b(W, s, r, n, d):
        ref = W.at[slot(offs[n], 0)]
        return remote(ref, ref, s.at[4 + 2 * n + d], r.at[4 + 2 * n + d], fb(1 if d == 0 else 3), t)

    def w_b2(W, s, r, n, d):
        ref = W.at[slot(offs[n], 3 if d == 0 else 1), hrows[d]]
        return remote(ref, ref, s.at[12 + 2 * n + d], r.at[12 + 2 * n + d], fb(1 if d == 0 else 3), t)

    def pump_a0(W, s, r):
        for d in (0, 1):
            w_a0(W, s, r, d).start()

    def pump_b(W, s, r, n):
        for d in (0, 1):
            w_b(W, s, r, n, d).start()

    def pump_a1(W, s, r):
        for d in (0, 1):
            w_a0(W, s, r, d).wait_recv()
        for d in (0, 1):
            w_a2(W, s, r, d).start()

    def pump_a2(W, s, r):
        for d in (0, 1):
            w_a2(W, s, r, d).wait_recv()

    def pump_b1(W, s, r, n):
        for d in (0, 1):
            w_b(W, s, r, n, d).wait_recv()
            w_b2(W, s, r, n, d).start()

    def pump_b2(W, s, r, n):
        for d in (0, 1):
            w_b2(W, s, r, n, d).wait_recv()

    U = (UB, us, ur)
    V = (DB, ds_, dr)
    pump_a0(*U)
    pump_b(*U, 0)
    pump_a0(*V)

    ph("d_wait_pa")
    for e in (1, 3, 2):
        p_a(e).wait_recv()
    for e in (1, 3, 2):
        p_b(e).start()
    ph("d_relay")
    relay_out().wait_recv()
    for k in (0, 1):
        relay_on(k).start()
    ph("e_U_a1")
    pump_a1(*U)
    pump_b(*U, 1)
    pump_b(*U, 2)

    def row_of(ref):
        return jnp.concatenate([ref[pl.ds(2 * t, 1), :], ref[pl.ds(2 * t + 1, 1), :]], axis=1)

    gm = row_of(gmix)
    NB[pl.ds(0, 16), :] = jnp.zeros((16, 256), BF16)
    NB[pl.ds(16 + SEQ, 16), :] = jnp.zeros((16, 256), BF16)
    ph("f_wait_x")
    c_x.wait()
    for e in range(1, 8):
        r_x(e).wait_recv()
    for n in range(5):
        near_in(n).wait()
    for k in (0, 1):
        relay_in(k).wait()
    ph("g_normed")
    for i in range(8):
        rc = to_column(R[i, 0:1, :])
        xv = X[pl.ds(128 * i, 128), :].astype(F32)
        NB[pl.ds(16 + 128 * i, 128), :] = (xv * rc * gm).astype(BF16)

    reach = 1 + (y >= 1).astype(jnp.int32) + 2 * (y >= 2).astype(jnp.int32) + 4 * (y >= 3).astype(jnp.int32)
    bi = lax.broadcasted_iota(jnp.int32, (128, 160), 0)
    bj = lax.broadcasted_iota(jnp.int32, (128, 160), 1)
    delta = bj - 16 - bi
    band = jnp.where((delta >= -reach) & (delta < reach), 1.0, 0.0).astype(BF16)

    def pl_x(q):
        ref = PL2.at[c, pl.ds(CH * q, CH)]
        return remote(ref, ref, xs.at[q], xr.at[q], f, sib)

    ph("h_pool")
    for i in range(8):
        sums = jnp.dot(band, NB[pl.ds(128 * i, 160), :], preferred_element_type=F32)
        pos = 128 * i + lax.broadcasted_iota(jnp.int32, (128, 256), 0)
        count = jnp.minimum(pos + reach, SEQ) - jnp.maximum(pos - reach, 0)
        mine = NB[pl.ds(16 + 128 * i, 128), :].astype(F32)
        PL2[c, pl.ds(128 * i, 128), :] = (sums / count.astype(F32) - mine).astype(BF16)
        if i % 2 == 1:
            pl_x(i // 2).start()

    ph("i_pb")
    for e in (1, 3, 2):
        p_b(e).wait_recv()
    ph("j_mix")
    psc = row_of(pscale)
    gml = row_of(gmlp)

    def g_ref(owner, q):
        return G.at[owner, pl.ds(CH * q, CH)]

    def g_y(q, d):
        return remote(g_ref(t, q), g_ref(t, q), gs.at[2 * q + d], gr.at[2 * q + d], f, yp if d == 0 else ym)

    def g_sib(k, q):
        owner = (t + (0, 6, 2, 4)[k]) % 8
        return remote(g_ref(owner, q), g_ref(owner, q), gs.at[8 + 4 * k + q], gr.at[8 + 4 * k + q], f, sib)

    def g_fwd(q):
        owner = ym if q < 2 else yp
        return remote(g_ref(owner, q), g_ref(owner, q), gs.at[24 + q], gr.at[24 + q], f, yp if q < 2 else ym)

    pk = [jnp.concatenate([PB[slot_of(8 * k + i)] for i in range(8)], axis=0) for k in (0, 1)]
    for q in range(NCH):
        pl_x(q).wait_recv()
        rows = pl.ds(CH * q, CH)
        mixed = (jnp.dot(PL2[0, rows, :], pk[0], preferred_element_type=F32)
                 + jnp.dot(PL2[1, rows, :], pk[1], preferred_element_type=F32)) * psc
        first = (X[rows, :].astype(F32) + mixed).astype(BF16).astype(F32)
        G[t, rows, :] = (first * gml).astype(BF16)
        for d in (0, 1):
            g_y(q, d).start()
        g_sib(0, q).start()
        ACC[0, rows, :] = first[:, :128]
        ACC[1, rows, :] = first[:, 128:]
        sq = jnp.sum(first * first, axis=1, keepdims=True)
        for h in (0, 1):
            SQ[t, pl.ds(2 * q + h, 1), :] = to_lanes(sq[128 * h:128 * h + 128])

    ph("k_sq")
    def sq_x(e):
        return remote(SQ.at[t], SQ.at[t], ss.at[e - 1], sr.at[e - 1], f, (t + e) % 8)

    for e in range(1, 8):
        sq_x(e).start()

    def g_pump(q):
        g_y(q, 0).wait_recv()
        if q < 2:
            g_fwd(q).start()
        g_sib(1, q).start()
        g_y(q, 1).wait_recv()
        if q >= 2:
            g_fwd(q).start()
        g_sib(2, q).start()

    def g_pump2(q):
        g_fwd(q).wait_recv()
        g_sib(3, q).start()

    ph("l_Ua2")
    pump_a2(*U)
    pump_b(*U, 3)
    pump_b1(*U, 0)
    ph("l_Va1")
    pump_a1(*V)
    ph("m_Ub1")
    pump_b1(*U, 1)
    ph("m_g0")
    g_pump(0)
    ph("m_Ub2")
    pump_b1(*U, 2)
    ph("m_g1")
    g_pump(1)
    ph("n_Ub3")
    pump_b1(*U, 3)
    pump_b(*V, 0)
    pump_b(*V, 1)
    ph("n_Va2")
    pump_a2(*V)

    @pl.when(c == 1)
    def _():
        pump_b(*V, 2)
        pump_b(*V, 3)

    ph("o_g2")
    g_pump(2)
    ph("o_g3")
    g_pump(3)
    ph("o_g20")
    g_pump2(0)
    g_pump2(2)
    ph("p_Ub2")
    for n in range(4):
        pump_b2(*U, n)
    for e in range(1, 8):
        sq_x(e).wait_recv()
    total = SQ[0]
    for i in range(1, 8):
        total = total + SQ[i]
    RT[...] = lax.rsqrt(total / D + EPS)

    def up_rows(q):
        for k in range(4):
            g_sib(k, q).wait_recv()
        ph(f"t_up{q}")
        rows = pl.ds(CH * q, CH)
        rc = jnp.concatenate([to_column(RT[2 * q + h:2 * q + h + 1, :]) for h in (0, 1)], axis=0)
        lhs = jnp.concatenate([G[i, rows, :] for i in range(8)], axis=1)
        rhs = jnp.concatenate([UB[slot_of(g)] for g in range(16)], axis=1)
        pre = lax.dot_general(lhs, rhs, (((1,), (1,)), ((), ())), preferred_element_type=F32)
        act = jnp.maximum(pre * rc, 0.0)
        H[rows, :] = (act * act).astype(BF16)

    ph("s_gsib0")
    up_rows(0)
    ph("u_Vb0")
    pump_b1(*V, 0)

    @pl.when(c == 0)
    def _():
        pump_b(*V, 2)

    ph("s_gsib2")
    up_rows(2)
    ph("s_g21")
    g_pump2(1)
    g_pump2(3)
    ph("s_gsib1")
    up_rows(1)
    ph("u_Vb1")
    pump_b1(*V, 1)

    @pl.when(c == 0)
    def _():
        pump_b(*V, 3)

    ph("s_gsib3")
    up_rows(3)

    ph("w_down")
    def c_x2(k, d):
        return remote(SO.at[k, d], SB.at[k, d], cs.at[4 * k + d], cr.at[4 * k + d], f, sib)

    def y_half(k, d):
        return remote(SO.at[k, 2, hrows[d]], RH.at[k, d], ys.at[4 * k + d], yr.at[4 * k + d], f, yp if d == 0 else ym)

    def y_now(k, d):
        return remote(SO.at[k, 1 + 2 * d, hrows[1 - d]], RY.at[k, d, hrows[1 - d]], ys.at[4 * k + 2 + d],
                      yr.at[4 * k + 2 + d], f, yp if d == 0 else ym)

    def y_late(k, d):
        return remote(SO.at[k, 1 + 2 * d, hrows[d]], RY.at[k, d, hrows[d]], ys.at[16 + 2 * k + d],
                      yr.at[16 + 2 * k + d], f, yp if d == 0 else ym)

    def ready(k):
        @pl.when(c == 0)
        def _():
            if k >= 2:
                pump_b1(*V, k)
            pump_b2(*V, k)

        @pl.when(c == 1)
        def _():
            if k == 1:
                pump_b1(*V, 2)
                pump_b1(*V, 3)
            if k == 3:
                for n in range(4):
                    pump_b2(*V, n)

    def roles(k):
        xk = (x + offs[k]) % 4
        return xk, xk // 2 == c, xk // 2 != c

    def down(k):
        xk, _, _ = roles(k)
        rhs = jnp.concatenate([DB[slot_of(4 * ((y + d) % 4) + xk)] for d in range(4)], axis=1)
        PART[k % 2] = jnp.dot(H[...], rhs, preferred_element_type=F32)

    def both(k, d, rows):
        return PART[k % 2, rows, 128 * d:128 * d + 128] + SB[k, d, rows].astype(F32)

    def stage1(k):
        _, owner, helper = roles(k)

        @pl.when(helper)
        def _():
            for d in (2, 1, 3, 0):
                SO[k, d] = PART[k % 2, :, 128 * d:128 * d + 128].astype(BF16)
                c_x2(k, d).start()

        @pl.when(owner)
        def _():
            c_x2(k, 2).wait_recv()
            for d in (0, 1):
                SO[k, 2, hrows[d]] = both(k, 2, hrows[d]).astype(BF16)
                y_half(k, d).start()
            for d in (0, 1):
                c_x2(k, 1 + 2 * d).wait_recv()
                SO[k, 1 + 2 * d, hrows[1 - d]] = both(k, 1 + 2 * d, hrows[1 - d]).astype(BF16)
                y_now(k, d).start()

    def stage2(k):
        xk, owner, _ = roles(k)

        @pl.when(owner)
        def _():
            for d in (0, 1):
                y_half(k, d).wait_recv()
                SO[k, 1 + 2 * d, hrows[d]] = (both(k, 1 + 2 * d, hrows[d]) + RH[k, d].astype(F32)).astype(BF16)
                y_late(k, d).start()
            c_x2(k, 0).wait_recv()
            for h in (0, 1):
                ACC[xk % 2, hrows[h]] = ACC[xk % 2, hrows[h]] + both(k, 0, hrows[h])

    def stage3(k):
        xk, owner, _ = roles(k)

        @pl.when(owner)
        def _():
            for d in (0, 1):
                y_now(k, d).wait_recv()
                y_late(k, d).wait_recv()
            ACC[xk % 2] = ACC[xk % 2] + RY[k, 0].astype(F32) + RY[k, 1].astype(F32)

    for step in ("r0", "d0", "10", "20", "r1", "d1", "11", "r2", "d2", "21", "12", "r3", "22", "d3", "13",
                 "30", "31", "32", "23", "33"):
        k = int(step[1])
        ph("w_" + step)
        {"r": ready, "d": down, "1": stage1, "2": stage2, "3": stage3}[step[0]](k)

    ph("y_sq2")
    for i in range(8):
        rows = pl.ds(128 * i, 128)
        a0, a1 = ACC[0, rows, :], ACC[1, rows, :]
        SQ2[t, pl.ds(i, 1), :] = to_lanes(jnp.sum(a0 * a0 + a1 * a1, axis=1, keepdims=True))

    def t_x(e):
        return remote(SQ2.at[t], SQ2.at[t], ts.at[e - 1], tr.at[e - 1], f, (t + e) % 8)

    for e in range(1, 8):
        t_x(e).start()
    ph("y_wait")
    for e in range(1, 8):
        t_x(e).wait_recv()
    total = SQ2[0]
    for i in range(1, 8):
        total = total + SQ2[i]
    rl = lax.rsqrt(total / D + EPS)
    for i in range(8):
        rows = pl.ds(128 * i, 128)
        rc = to_column(rl[i:i + 1, :])
        for h in (0, 1):
            out[rows, 128 * h:128 * h + 128] = (ACC[h, rows, :] * rc * gout[h:h + 1, :]).astype(BF16)

    ph("z_sent")
    relay_out().wait_send()
    for k in (0, 1):
        relay_on(k).wait_send()
    for n in range(5):
        near(n).wait_send()
    for e in range(1, 8):
        r_x(e).wait_send()
        sq_x(e).wait_send()
        t_x(e).wait_send()
    for k in range(4):
        _, owner, helper = roles(k)

        @pl.when(owner)
        def _():
            for d in (0, 1):
                y_half(k, d).wait_send()
                y_now(k, d).wait_send()
                y_late(k, d).wait_send()

        @pl.when(helper)
        def _():
            for d in range(4):
                c_x2(k, d).wait_send()

    for e in (1, 2, 3):
        p_a(e).wait_send()
        p_b(e).wait_send()
    for W in (U, V):
        for d in (0, 1):
            w_a0(*W, d).wait_send()
            w_a2(*W, d).wait_send()
            for n in range(4):
                w_b(*W, n, d).wait_send()
                w_b2(*W, n, d).wait_send()
    for q in range(NCH):
        pl_x(q).wait_send()
        g_y(q, 0).wait_send()
        g_y(q, 1).wait_send()
        g_fwd(q).wait_send()
        for k in range(4):
            g_sib(k, q).wait_send()
    ph(None)


def local(tokens, pool_weight, pool_scale, gain_mix, gain_mlp, w_up, w_down, gain_out):
    dma = pltpu.SemaphoreType.DMA
    hbm = pl.BlockSpec(memory_space=pl.ANY)
    vmem = pl.BlockSpec(memory_space=pltpu.VMEM)
    return pl.pallas_call(
        kernel,
        out_shape=jax.ShapeDtypeStruct((SEQ, 256), BF16),
        in_specs=[hbm] * 4 + [vmem] * 4,
        out_specs=vmem,
        scratch_shapes=[
            pltpu.VMEM((128, D), BF16),
            pltpu.VMEM((128, 512), BF16),
            pltpu.VMEM((SEQ, 256), BF16),
            pltpu.VMEM((SEQ + 32, 256), BF16),
            pltpu.VMEM((8, 8, 128), F32),
            pltpu.VMEM((8, 128), F32),
            pltpu.VMEM((16, 32, 256), BF16),
            pltpu.VMEM((16, 1024, 128), BF16),
            pltpu.VMEM((16, 1024, 128), BF16),
            pltpu.VMEM((2, SEQ, 256), BF16),
            pltpu.VMEM((8, SEQ, 256), BF16),
            pltpu.VMEM((8, 8, 128), F32),
            pltpu.VMEM((8, 8, 128), F32),
            pltpu.VMEM((SEQ, 1024), BF16),
            pltpu.VMEM((2, SEQ, 512), F32),
            pltpu.VMEM((4, 4, SEQ, 128), BF16),
            pltpu.VMEM((4, 4, SEQ, 128), BF16),
            pltpu.VMEM((4, 2, HALF, 128), BF16),
            pltpu.VMEM((4, 2, SEQ, 128), BF16),
            pltpu.VMEM((2, SEQ, 128), F32),
            dma((5,)),
            dma((8,)), dma((8,)),
            dma((7,)), dma((7,)),
            dma((6,)), dma((6,)),
            dma((20,)), dma((20,)),
            dma((20,)), dma((20,)),
            dma((4,)), dma((4,)),
            dma((28,)), dma((28,)),
            dma((7,)), dma((7,)),
            dma((7,)), dma((7,)),
            dma((16,)), dma((16,)),
            dma((24,)), dma((24,)),
        ],
        compiler_params=pltpu.CompilerParams(
            collective_id=0, has_side_effects=True, vmem_limit_bytes=60 * 1024 * 1024),
        name="mixers",
    )(tokens, pool_weight, w_up, w_down, pool_scale.reshape(16, 128), gain_mix.reshape(16, 128),
      gain_mlp.reshape(16, 128), gain_out.reshape(2, 128))


def solution(mesh):
    placed = (P(("fs", "tp"), None), P(None, "fs", None), P(), P(), P(), P("tp", "fs"), P("tp", "fs"), P("tp"))
    return jax.shard_map(local, mesh=mesh, in_specs=placed, out_specs=P("fs", "tp"), check_vma=False)
```

```python
import functools

import jax
import jax.numpy as jnp
from jax import lax
from jax.experimental import pallas as pl
from jax.experimental.pallas import tpu as pltpu
from jax.sharding import PartitionSpec as P

D = 2048
SEQ = 1024
EPS = 1e-06
F32 = jnp.float32
BF16 = jnp.bfloat16
MESH = pl.DeviceIdType.MESH
CH = 256
NCH = SEQ // CH
HALF = SEQ // 2


class Phases:
    now = None

    def __call__(self, name):
        if self.now is not None:
            self.now.__exit__(None, None, None)
        self.now = jax.named_scope(name) if name else None
        if name:
            self.now.__enter__()


def kernel(tok, pw, up, dn, pscale_h, gmix_h, gmlp_h, gout_h, out,
           tokv, RL, X, NB, R, RT, PB, UB, DB, PL2, G, SQ, SQ2, H, PART, SS, SB, SO, RH, RY, RZ, ACC,
           pscale, gmix, gmlp, gout, lsem, snd, rcv):
    ph = Phases()
    f = lax.axis_index("fs")
    t = lax.axis_index("tp")
    z, x = f // 4, f % 4
    y, c = t // 2, t % 2

    def fa(d):
        return (1 - c) * (4 * z + (x + d) % 4) + c * (4 * ((z + d) % 4) + x)

    def fb(d):
        return (1 - c) * (4 * ((z + d) % 4) + x) + c * (4 * z + (x + d) % 4)

    pa = (1 - c) * x + c * z
    pb = (1 - c) * z + c * x

    def slot(i, j):
        return 4 * ((pb + j) % 4) + (pa + i) % 4

    def slot_of(g):
        return (1 - c) * g + c * (4 * (g % 4) + g // 4)

    def remote(src, dst, ssem, rsem, fs, tp):
        return pltpu.make_async_remote_copy(
            src_ref=src, dst_ref=dst, send_sem=snd.at[ssem], recv_sem=rcv.at[rsem],
            device_id={"fs": fs, "tp": tp}, device_id_type=MESH)

    def arrived(ref, rsem):
        pltpu.make_async_copy(ref, ref, rcv.at[rsem]).wait()

    sib = 2 * y + 1 - c
    yp = 2 * ((y + 1) % 4) + c
    ym = 2 * ((y + 3) % 4) + c
    own = slot(0, 0)

    ph("a_entry")
    c_tok = pltpu.make_async_copy(tok, tokv, lsem.at[0])
    c_x = pltpu.make_async_copy(
        tok.at[:, pl.ds(pl.multiple_of(256 * t, 256), 256)],
        X.at[pl.ds(pl.multiple_of(128 * t, 128), 128)], lsem.at[1])
    c_u = pltpu.make_async_copy(up, UB.at[own], lsem.at[2])
    c_d = pltpu.make_async_copy(dn, DB.at[own], lsem.at[3])
    c_p = pltpu.make_async_copy(
        pw.at[y, :, pl.ds(pl.multiple_of(256 * c, 256), 256)], PB.at[own], lsem.at[4])
    c_g = [pltpu.make_async_copy(h, v, lsem.at[5 + i])
           for i, (h, v) in enumerate(((pscale_h, pscale), (gmix_h, gmix), (gmlp_h, gmlp), (gout_h, gout)))]
    for cp in [c_tok, c_p, c_u, c_x, c_d] + c_g:
        cp.start()
    barrier = pltpu.get_barrier_semaphore()
    for e in range(1, 8):
        pl.semaphore_signal(barrier, inc=1, device_id={"fs": f, "tp": (t + e) % 8}, device_id_type=MESH)
    for e in (1, 2, 3):
        pl.semaphore_signal(barrier, inc=1, device_id={"fs": fa(e), "tp": t}, device_id_type=MESH)
        pl.semaphore_signal(barrier, inc=1, device_id={"fs": fb(e), "tp": t}, device_id_type=MESH)

    ri = lax.broadcasted_iota(jnp.int32, (128, 128), 0)
    ci = lax.broadcasted_iota(jnp.int32, (128, 128), 1)
    eye = (ri == ci).astype(F32)

    def to_lanes(col):
        return jnp.sum(col * eye, axis=0, keepdims=True)

    def to_column(lanes):
        return jnp.sum(lanes * eye, axis=1, keepdims=True)

    c_tok.wait()
    v = tokv[...].astype(F32)
    r1 = lax.rsqrt(jnp.sum(v * v, axis=1, keepdims=True) / D + EPS)
    R[t] = jnp.broadcast_to(to_lanes(r1), (8, 128))
    c_p.wait()
    c_u.wait()
    c_d.wait()
    pl.semaphore_wait(barrier, 13)

    ph("b_start")
    via = (y + 1 + 2 * c) % 4

    def rows_of(o):
        return pl.ds(pl.multiple_of(128 * o, 128), 128)

    def near(n):
        p = (2 * ((y + (1 if n < 2 else 3)) % 4) + n % 2) if n < 4 else sib
        return remote(tokv.at[:, pl.ds(pl.multiple_of(256 * p, 256), 256)], X.at[rows_of(t)], 0, 0, f, p)

    def relay_out():
        return remote(tokv.at[:, pl.ds(pl.multiple_of(512 * ((y + 2) % 4), 512), 512)], RL, 0, 1, f, 2 * via + c)

    def relay_on(k):
        o = 2 * ((y + 3 + 2 * c) % 4) + c
        return remote(RL.at[:, pl.ds(256 * k, 256)], X.at[rows_of(o)], 0, 0, f, 2 * via + k)

    relay_out().start()
    for n in (0, 2, 1, 3, 4):
        near(n).start()

    def r_x(e):
        return remote(R.at[t], R.at[t], 1, 2, f, (t + e) % 8)

    for e in range(1, 8):
        r_x(e).start()

    def p_a(e):
        return remote(PB.at[own], PB.at[own], 1, 3, fa(e), t)

    def p_b(e):
        line = PB.at[pl.ds(4 * pb, 4)]
        return remote(line, line, 1, 4, fb(e), t)

    for e in (1, 3, 2):
        p_a(e).start()

    hrows = (pl.ds(0, HALF), pl.ds(HALF, HALF))
    offs = (0, 3, 1, 2)

    def w_a0(W, s, r, d):
        ref = W.at[own]
        return remote(ref, ref, s, r, fa(1 if d == 0 else 3), t)

    def w_a2(W, s, r, d):
        ref = W.at[slot(3 if d == 0 else 1, 0), hrows[d]]
        return remote(ref, ref, s, r + 1, fa(1 if d == 0 else 3), t)

    def w_b(W, s, r, n, d):
        ref = W.at[slot(offs[n], 0)]
        return remote(ref, ref, s, r + 2 + n, fb(1 if d == 0 else 3), t)

    def w_b2(W, s, r, n, d):
        ref = W.at[slot(offs[n], 3 if d == 0 else 1), hrows[d]]
        return remote(ref, ref, s, r + 6 + n, fb(1 if d == 0 else 3), t)

    def pump_a0(W, s, r):
        for d in (0, 1):
            w_a0(W, s, r, d).start()

    def pump_b(W, s, r, n):
        for d in (0, 1):
            w_b(W, s, r, n, d).start()

    def pump_a1(W, s, r):
        arrived(W.at[pl.ds(0, 2)], r)
        for d in (0, 1):
            w_a2(W, s, r, d).start()

    def pump_a2(W, s, r):
        arrived(W.at[0], r + 1)

    def pump_b1(W, s, r, n):
        arrived(W.at[pl.ds(0, 2)], r + 2 + n)
        for d in (0, 1):
            w_b2(W, s, r, n, d).start()

    def pump_b2(W, s, r, n):
        arrived(W.at[0], r + 6 + n)

    U = (UB, 2, 5)
    V = (DB, 3, 15)
    pump_a0(*U)
    pump_b(*U, 0)

    ph("d_wait_pa")
    arrived(PB.at[pl.ds(0, 3)], 3)
    for e in (1, 3, 2):
        p_b(e).start()
    ph("d_relay")
    arrived(RL, 1)
    for k in (0, 1):
        relay_on(k).start()
    ph("e_Ua1")
    pump_a1(*U)
    pump_b(*U, 1)
    pump_b(*U, 2)
    def row_of(ref):
        return jnp.concatenate([ref[pl.ds(2 * t, 1), :], ref[pl.ds(2 * t + 1, 1), :]], axis=1)

    NB[pl.ds(0, 16), :] = jnp.zeros((16, 256), BF16)
    NB[pl.ds(16 + SEQ, 16), :] = jnp.zeros((16, 256), BF16)
    ph("f_wait_x")
    c_x.wait()
    for cp in c_g:
        cp.wait()
    gm = row_of(gmix)
    arrived(R.at[pl.ds(0, 7)], 2)
    arrived(X.at[pl.ds(0, 896)], 0)
    ph("g_normed")
    for i in range(8):
        rc = to_column(R[i, 0:1, :])
        xv = X[pl.ds(128 * i, 128), :].astype(F32)
        NB[pl.ds(16 + 128 * i, 128), :] = (xv * rc * gm).astype(BF16)

    reach = 1 + (y >= 1).astype(jnp.int32) + 2 * (y >= 2).astype(jnp.int32) + 4 * (y >= 3).astype(jnp.int32)
    bi = lax.broadcasted_iota(jnp.int32, (128, 160), 0)
    bj = lax.broadcasted_iota(jnp.int32, (128, 160), 1)
    delta = bj - 16 - bi
    band = jnp.where((delta >= -reach) & (delta < reach), 1.0, 0.0).astype(BF16)

    def pl_x(q):
        ref = PL2.at[c, pl.ds(CH * q, CH)]
        return remote(ref, ref, 4, 25 + q, f, sib)

    ph("h_pool")
    for i in range(8):
        sums = jnp.dot(band, NB[pl.ds(128 * i, 160), :], preferred_element_type=F32)
        pos = 128 * i + lax.broadcasted_iota(jnp.int32, (128, 256), 0)
        count = jnp.minimum(pos + reach, SEQ) - jnp.maximum(pos - reach, 0)
        mine = NB[pl.ds(16 + 128 * i, 128), :].astype(F32)
        PL2[c, pl.ds(128 * i, 128), :] = (sums / count.astype(F32) - mine).astype(BF16)
        if i % 2 == 1:
            pl_x(i // 2).start()

    ph("i_pb")
    arrived(PB.at[pl.ds(0, 12)], 4)
    ph("j_mix")
    psc = row_of(pscale)
    gml = row_of(gmlp)

    def g_ref(owner, q):
        return G.at[owner, pl.ds(CH * q, CH)]

    def g_y(q, d):
        return remote(g_ref(t, q), g_ref(t, q), 5, 29 + q, f, yp if d == 0 else ym)

    def g_sib(k, q):
        owner = (t + (0, 6, 2, 4)[k]) % 8
        return remote(g_ref(owner, q), g_ref(owner, q), 5, 35 + q, f, sib)

    def g_fwd(q):
        owner = ym if q < 2 else yp
        return remote(g_ref(owner, q), g_ref(owner, q), 5, 33 + q % 2, f, yp if q < 2 else ym)

    pk = [jnp.concatenate([PB[slot_of(8 * k + i)] for i in range(8)], axis=0) for k in (0, 1)]
    for q in range(NCH):
        arrived(PL2.at[1 - c, pl.ds(CH * q, CH)], 25 + q)
        rows = pl.ds(CH * q, CH)
        mixed = (jnp.dot(PL2[0, rows, :], pk[0], preferred_element_type=F32)
                 + jnp.dot(PL2[1, rows, :], pk[1], preferred_element_type=F32)) * psc
        first = (X[rows, :].astype(F32) + mixed).astype(BF16).astype(F32)
        G[t, rows, :] = (first * gml).astype(BF16)
        for d in (0, 1):
            g_y(q, d).start()
        g_sib(0, q).start()
        ACC[0, rows, :] = first[:, :128]
        ACC[1, rows, :] = first[:, 128:]
        sq = jnp.sum(first * first, axis=1, keepdims=True)
        for h in (0, 1):
            SQ[t, pl.ds(2 * q + h, 1), :] = to_lanes(sq[128 * h:128 * h + 128])

    ph("k_sq")
    def sq_x(e):
        return remote(SQ.at[t], SQ.at[t], 1, 39, f, (t + e) % 8)

    for e in range(1, 8):
        sq_x(e).start()

    def g_pump(q):
        arrived(G.at[0, pl.ds(0, 2 * CH)], 29 + q)
        g_fwd(q).start()
        g_sib(1, q).start()
        g_sib(2, q).start()

    def g_pump2(q):
        arrived(G.at[0, pl.ds(0, 2 * CH)], 33 + q)
        g_sib(3, q).start()
        g_sib(3, q + 2).start()

    ph("l_Ub0")
    pump_b1(*U, 0)
    ph("l_Ua2")
    pump_a2(*U)
    pump_b(*U, 3)
    ph("m_Ub1")
    pump_b1(*U, 1)
    pump_a0(*V)
    ph("m_g0")
    g_pump(0)
    ph("m_g1")
    g_pump(1)
    ph("m_Ub2")
    pump_b1(*U, 2)
    ph("m_g2")
    g_pump(2)
    ph("n_Ub3")
    pump_b1(*U, 3)
    pump_b(*V, 0)
    ph("n_Va1")
    pump_a1(*V)
    pump_b(*V, 1)

    @pl.when(c == 1)
    def _():
        pump_b(*V, 2)

    ph("o_g3")
    g_pump(3)
    ph("o_g20")
    g_pump2(0)
    ph("p_Ub2")
    for n in range(4):
        pump_b2(*U, n)
    ph("p_g21")
    g_pump2(1)
    ph("p_Va2")
    pump_a2(*V)

    @pl.when(c == 1)
    def _():
        pump_b(*V, 3)

    arrived(SQ.at[pl.ds(0, 7)], 39)
    total = SQ[0]
    for i in range(1, 8):
        total = total + SQ[i]
    RT[...] = lax.rsqrt(total / D + EPS)

    def up_rows(q):
        arrived(G.at[pl.ds(0, 4), pl.ds(0, CH)], 35 + q)
        ph(f"t_up{q}")
        rows = pl.ds(CH * q, CH)
        rc = jnp.concatenate([to_column(RT[2 * q + h:2 * q + h + 1, :]) for h in (0, 1)], axis=0)
        lhs = jnp.concatenate([G[i, rows, :] for i in range(8)], axis=1)
        rhs = jnp.concatenate([UB[slot_of(g)] for g in range(16)], axis=1)
        pre = lax.dot_general(lhs, rhs, (((1,), (1,)), ((), ())), preferred_element_type=F32)
        act = jnp.maximum(pre * rc, 0.0)
        H[rows, :] = (act * act).astype(BF16)

    ph("s_gsib0")
    up_rows(0)
    ph("s_gsib2")
    up_rows(2)
    ph("u_Vb0")
    pump_b1(*V, 0)

    @pl.when(c == 0)
    def _():
        pump_b(*V, 2)

    ph("s_gsib1")
    up_rows(1)
    ph("u_Vb1")
    pump_b1(*V, 1)

    @pl.when(c == 0)
    def _():
        pump_b(*V, 3)

    ph("s_gsib3")
    up_rows(3)

    mine, other = pl.ds(pl.multiple_of(HALF * c, HALF), HALF), pl.ds(pl.multiple_of(HALF * (1 - c), HALF), HALF)
    quarter = HALF // 2
    qrows = (pl.ds(0, quarter), pl.ds(quarter, quarter))

    def column(k):
        xk = (x + offs[k]) % 4
        return xk, xk // 2

    def c_x2(k, d):
        return remote(SS.at[k, d], SB.at[k, d], 4, 40 + 4 * k + d, f, sib)

    def y_half(k, d):
        return remote(SO.at[k, 2, qrows[d]], RH.at[k, d], 6, 56 + 2 * k + d, f, yp if d == 0 else ym)

    def y_part(k, d, h):
        to = 2 * ((y + 1 + 2 * d) % 4) + column(k)[1]
        rows = pl.ds(pl.multiple_of(HALF * c + quarter * h, quarter), quarter)
        return remote(SO.at[k, 1 + 2 * d, qrows[h]], RY.at[k, d, rows], 6, 64 + k, f, to)

    def z_x(k):
        return remote(SO.at[k, 0], RZ.at[k], 4, 68 + k, f, sib)

    def ready(k):
        @pl.when(c == 0)
        def _():
            if k in (1, 2):
                pump_b1(*V, k + 1)
            pump_b2(*V, k)

        @pl.when(c == 1)
        def _():
            if k == 1:
                pump_b1(*V, 2)
                pump_b1(*V, 3)
            if k == 3:
                for n in range(4):
                    pump_b2(*V, n)

    def down(k):
        xk, _ = column(k)
        rhs = jnp.concatenate([DB[slot_of(4 * ((y + d) % 4) + xk)] for d in range(4)], axis=1)
        part = jnp.dot(H[other, :], rhs, preferred_element_type=F32)
        for d in (2, 1, 3, 0):
            SS[k, d] = part[:, 128 * d:128 * d + 128].astype(BF16)
            c_x2(k, d).start()
        PART[k % 2] = jnp.dot(H[mine, :], rhs, preferred_element_type=F32)

    def both(k, d, rows):
        return PART[k % 2, rows, 128 * d:128 * d + 128] + SB[k, d, rows].astype(F32)

    def stage1(k):
        arrived(SB.at[k, 2], 40 + 4 * k + 2)
        for d in (0, 1):
            SO[k, 2, qrows[d]] = both(k, 2, qrows[d]).astype(BF16)
            y_half(k, d).start()
        for d in (0, 1):
            b = 1 + 2 * d
            arrived(SB.at[k, b], 40 + 4 * k + b)
            SO[k, b, qrows[1 - d]] = both(k, b, qrows[1 - d]).astype(BF16)
            y_part(k, d, 1 - d).start()

    def stage2(k):
        xk, keeper = column(k)
        for d in (0, 1):
            b = 1 + 2 * d
            arrived(RH.at[k, d], 56 + 2 * k + d)
            SO[k, b, qrows[d]] = (both(k, b, qrows[d]) + RH[k, d].astype(F32)).astype(BF16)
            y_part(k, d, d).start()
        arrived(SB.at[k, 0], 40 + 4 * k)

        @pl.when(keeper == c)
        def _():
            ACC[xk % 2, mine] = ACC[xk % 2, mine] + both(k, 0, pl.ds(0, HALF))

        @pl.when(keeper != c)
        def _():
            SO[k, 0] = both(k, 0, pl.ds(0, HALF)).astype(BF16)
            z_x(k).start()

    def stage3(k):
        xk, keeper = column(k)

        @pl.when(keeper == c)
        def _():
            arrived(RZ.at[k], 68 + k)
            ACC[xk % 2, other] = ACC[xk % 2, other] + RZ[k].astype(F32)
            arrived(RY.at[k], 64 + k)
            ACC[xk % 2] = ACC[xk % 2] + RY[k, 0].astype(F32) + RY[k, 1].astype(F32)

    for step in ("r0", "d0", "10", "r1", "d1", "11", "20", "r2", "d2", "12", "21", "r3", "d3", "13",
                 "22", "30", "23", "31", "32", "33"):
        k = int(step[1])
        ph("w_" + step)
        {"r": ready, "d": down, "1": stage1, "2": stage2, "3": stage3}[step[0]](k)

    ph("y_sq2")
    for i in range(8):
        rows = pl.ds(128 * i, 128)
        a0, a1 = ACC[0, rows, :], ACC[1, rows, :]
        SQ2[t, pl.ds(i, 1), :] = to_lanes(jnp.sum(a0 * a0 + a1 * a1, axis=1, keepdims=True))

    def t_x(e):
        return remote(SQ2.at[t], SQ2.at[t], 1, 72, f, (t + e) % 8)

    for e in range(1, 8):
        t_x(e).start()
    ph("y_wait")
    arrived(SQ2.at[pl.ds(0, 7)], 72)
    total = SQ2[0]
    for i in range(1, 8):
        total = total + SQ2[i]
    rl = lax.rsqrt(total / D + EPS)

    def out_x(q):
        rows = pl.ds(CH * q, CH)
        return pltpu.make_async_copy(X.at[rows], out.at[rows], lsem.at[q])

    for i in range(8):
        rows = pl.ds(128 * i, 128)
        rc = to_column(rl[i:i + 1, :])
        for h in (0, 1):
            X[rows, 128 * h:128 * h + 128] = (ACC[h, rows, :] * rc * gout[h:h + 1, :]).astype(BF16)
        if i % 2 == 1:
            out_x(i // 2).start()

    ph("z_sent")
    relay_out().wait_send()
    for k in (0, 1):
        relay_on(k).wait_send()
    for n in range(5):
        near(n).wait_send()
    for e in range(1, 8):
        r_x(e).wait_send()
        sq_x(e).wait_send()
        t_x(e).wait_send()
    for e in (1, 2, 3):
        p_a(e).wait_send()
        p_b(e).wait_send()
    for W in (U, V):
        for d in (0, 1):
            w_a0(*W, d).wait_send()
            w_a2(*W, d).wait_send()
            for n in range(4):
                w_b(*W, n, d).wait_send()
                w_b2(*W, n, d).wait_send()
    for q in range(NCH):
        pl_x(q).wait_send()
        g_y(q, 0).wait_send()
        g_y(q, 1).wait_send()
        g_fwd(q).wait_send()
        for k in range(4):
            g_sib(k, q).wait_send()
    for k in range(4):
        for d in range(4):
            c_x2(k, d).wait_send()
        for d in (0, 1):
            y_half(k, d).wait_send()
            y_part(k, d, 0).wait_send()
            y_part(k, d, 1).wait_send()

        @pl.when(column(k)[1] != c)
        def _():
            z_x(k).wait_send()

    for q in range(NCH):
        out_x(q).wait()
    ph(None)


def local(tokens, pool_weight, pool_scale, gain_mix, gain_mlp, w_up, w_down, gain_out):
    dma = pltpu.SemaphoreType.DMA
    hbm = pl.BlockSpec(memory_space=pltpu.HBM)
    return pl.pallas_call(
        kernel,
        out_shape=jax.ShapeDtypeStruct((SEQ, 256), BF16),
        in_specs=[hbm] * 8,
        out_specs=hbm,
        scratch_shapes=[
            pltpu.VMEM((128, D), BF16),
            pltpu.VMEM((128, 512), BF16),
            pltpu.VMEM((SEQ, 256), BF16),
            pltpu.VMEM((SEQ + 32, 256), BF16),
            pltpu.VMEM((8, 8, 128), F32),
            pltpu.VMEM((8, 128), F32),
            pltpu.VMEM((16, 32, 256), BF16),
            pltpu.VMEM((16, 1024, 128), BF16),
            pltpu.VMEM((16, 1024, 128), BF16),
            pltpu.VMEM((2, SEQ, 256), BF16),
            pltpu.VMEM((8, SEQ, 256), BF16),
            pltpu.VMEM((8, 8, 128), F32),
            pltpu.VMEM((8, 8, 128), F32),
            pltpu.VMEM((SEQ, 1024), BF16),
            pltpu.VMEM((2, HALF, 512), F32),
            pltpu.VMEM((4, 4, HALF, 128), BF16),
            pltpu.VMEM((4, 4, HALF, 128), BF16),
            pltpu.VMEM((4, 4, HALF, 128), BF16),
            pltpu.VMEM((4, 2, HALF // 2, 128), BF16),
            pltpu.VMEM((4, 2, SEQ, 128), BF16),
            pltpu.VMEM((4, HALF, 128), BF16),
            pltpu.VMEM((2, SEQ, 128), F32),
            pltpu.VMEM((16, 128), F32),
            pltpu.VMEM((16, 128), F32),
            pltpu.VMEM((16, 128), F32),
            pltpu.VMEM((2, 128), F32),
            dma((9,)),
            dma((7,)),
            dma((73,)),
        ],
        compiler_params=pltpu.CompilerParams(
            collective_id=0, has_side_effects=True, vmem_limit_bytes=60 * 1024 * 1024),
        name="mixers",
    )(tokens, pool_weight, w_up, w_down, pool_scale.reshape(16, 128), gain_mix.reshape(16, 128),
      gain_mlp.reshape(16, 128), gain_out.reshape(2, 128))


def solution(mesh):
    placed = (P(("fs", "tp"), None), P(None, "fs", None), P(), P(), P(), P("tp", "fs"), P("tp", "fs"), P("tp"))
    return jax.shard_map(local, mesh=mesh, in_specs=placed, out_specs=P("fs", "tp"), check_vma=False)
```

```python
import functools

import jax
import jax.numpy as jnp
from jax import lax
from jax.experimental import pallas as pl
from jax.experimental.pallas import tpu as pltpu
from jax.sharding import PartitionSpec as P

D = 2048
SEQ = 1024
EPS = 1e-06
F32 = jnp.float32
BF16 = jnp.bfloat16
MESH = pl.DeviceIdType.MESH
CH = 256
NCH = SEQ // CH
HALF = SEQ // 2
J = 1
UR = HALF // J


class Phases:
    now = None

    def __call__(self, name):
        if self.now is not None:
            self.now.__exit__(None, None, None)
        self.now = jax.named_scope(name) if name else None
        if name:
            self.now.__enter__()


def kernel(tok, pw, up, dn, pscale_h, gmix_h, gmlp_h, gout_h, out,
           tokv, RL, HX, X, NB, R, RT, PB, UB, DB, PL2, G, SQ, SQ2, H, PART, SS, SB, SO, RH, RY, RZ, ACC,
           pscale, gmix, gmlp, gout, lsem, snd, rcv):
    ph = Phases()
    f = lax.axis_index("fs")
    t = lax.axis_index("tp")
    z, x = f // 4, f % 4
    y, c = t // 2, t % 2

    def fa(d):
        return (1 - c) * (4 * z + (x + d) % 4) + c * (4 * ((z + d) % 4) + x)

    def fb(d):
        return (1 - c) * (4 * ((z + d) % 4) + x) + c * (4 * z + (x + d) % 4)

    pa = (1 - c) * x + c * z
    pb = (1 - c) * z + c * x

    def slot(i, j):
        return 4 * ((pb + j) % 4) + (pa + i) % 4

    def slot_of(g):
        return (1 - c) * g + c * (4 * (g % 4) + g // 4)

    def remote(src, dst, ssem, rsem, fs, tp):
        return pltpu.make_async_remote_copy(
            src_ref=src, dst_ref=dst, send_sem=snd.at[ssem], recv_sem=rcv.at[rsem],
            device_id={"fs": fs, "tp": tp}, device_id_type=MESH)

    def arrived(ref, rsem):
        pltpu.make_async_copy(ref, ref, rcv.at[rsem]).wait()

    sib = 2 * y + 1 - c
    yp = 2 * ((y + 1) % 4) + c
    ym = 2 * ((y + 3) % 4) + c
    own = slot(0, 0)

    ph("a_entry")
    c_tok = pltpu.make_async_copy(tok, tokv, lsem.at[0])
    c_x = pltpu.make_async_copy(
        tok.at[:, pl.ds(pl.multiple_of(256 * t, 256), 256)],
        X.at[pl.ds(pl.multiple_of(128 * t, 128), 128)], lsem.at[1])
    c_u = pltpu.make_async_copy(up, UB.at[own], lsem.at[2])
    c_d = pltpu.make_async_copy(dn, DB.at[own], lsem.at[3])
    c_p = pltpu.make_async_copy(
        pw.at[y, :, pl.ds(pl.multiple_of(256 * c, 256), 256)], PB.at[own], lsem.at[4])
    c_g = [pltpu.make_async_copy(h, v, lsem.at[5 + i])
           for i, (h, v) in enumerate(((pscale_h, pscale), (gmix_h, gmix), (gmlp_h, gmlp), (gout_h, gout)))]
    for cp in [c_tok, c_p, c_u, c_x, c_d] + c_g:
        cp.start()
    barrier = pltpu.get_barrier_semaphore()
    for e in range(1, 8):
        pl.semaphore_signal(barrier, inc=1, device_id={"fs": f, "tp": (t + e) % 8}, device_id_type=MESH)
    for e in (1, 2, 3):
        pl.semaphore_signal(barrier, inc=1, device_id={"fs": fa(e), "tp": t}, device_id_type=MESH)
        pl.semaphore_signal(barrier, inc=1, device_id={"fs": fb(e), "tp": t}, device_id_type=MESH)

    ri = lax.broadcasted_iota(jnp.int32, (128, 128), 0)
    ci = lax.broadcasted_iota(jnp.int32, (128, 128), 1)
    eye = (ri == ci).astype(F32)

    def to_lanes(col):
        return jnp.sum(col * eye, axis=0, keepdims=True)

    def to_column(lanes):
        return jnp.sum(lanes * eye, axis=1, keepdims=True)

    c_tok.wait()
    v = tokv[...].astype(F32)
    r1 = lax.rsqrt(jnp.sum(v * v, axis=1, keepdims=True) / D + EPS)
    R[t] = jnp.broadcast_to(to_lanes(r1), (8, 128))
    c_p.wait()
    c_u.wait()
    c_d.wait()
    pl.semaphore_wait(barrier, 13)

    ph("b_start")
    via = (y + 1 + 2 * c) % 4

    def rows_of(o):
        return pl.ds(pl.multiple_of(128 * o, 128), 128)

    def near(n):
        p = (2 * ((y + (1 if n < 2 else 3)) % 4) + n % 2) if n < 4 else sib
        return remote(tokv.at[:, pl.ds(pl.multiple_of(256 * p, 256), 256)], X.at[rows_of(t)], 0, 0, f, p)

    def relay_out():
        return remote(tokv.at[:, pl.ds(pl.multiple_of(512 * ((y + 2) % 4), 512), 512)], RL, 0, 1, f, 2 * via + c)

    def relay_on(k):
        o = 2 * ((y + 3 + 2 * c) % 4) + c
        return remote(RL.at[:, pl.ds(256 * k, 256)], X.at[rows_of(o)], 0, 19, f, 2 * via + k)

    def edge(k):
        p = 2 * ((y + 2) % 4) + k
        return remote(tokv.at[pl.ds(pl.multiple_of(112 * c, 16), 16), pl.ds(pl.multiple_of(256 * p, 256), 256)],
                      HX.at[c], 0, 20, f, p)

    for k in (0, 1):
        edge(k).start()
    relay_out().start()
    for n in (0, 2, 1, 3, 4):
        near(n).start()

    def r_x(e):
        return remote(R.at[t], R.at[t], 1, 2, f, (t + e) % 8)

    for e in range(1, 8):
        r_x(e).start()

    def p_a(e):
        return remote(PB.at[own], PB.at[own], 1, 3, fa(e), t)

    def p_b(e):
        line = PB.at[pl.ds(4 * pb, 4)]
        return remote(line, line, 1, 4, fb(e), t)

    for e in (1, 3, 2):
        p_a(e).start()

    hrows = (pl.ds(0, HALF), pl.ds(HALF, HALF))
    offs = (0, 3, 1, 2)

    def w_a0(W, s, r, d):
        ref = W.at[own]
        return remote(ref, ref, s, r, fa(1 if d == 0 else 3), t)

    def w_a2(W, s, r, d):
        ref = W.at[slot(3 if d == 0 else 1, 0), hrows[d]]
        return remote(ref, ref, s, r + 1, fa(1 if d == 0 else 3), t)

    def w_b(W, s, r, n, d, h):
        ref = W.at[slot(offs[n], 0)] if h == 2 else W.at[slot(offs[n], 0), hrows[d if h == 0 else 1 - d]]
        return remote(ref, ref, s, r + (10 if h == 1 else 2) + n, fb(1 if d == 0 else 3), t)

    def w_b2(W, s, r, n, d):
        ref = W.at[slot(offs[n], 3 if d == 0 else 1), hrows[d]]
        return remote(ref, ref, s, r + 6 + n, fb(1 if d == 0 else 3), t)

    def pump_a0(W, s, r):
        for d in (0, 1):
            w_a0(W, s, r, d).start()

    def pump_bh(W, s, r, n, h):
        for d in (0, 1):
            w_b(W, s, r, n, d, h).start()

    def pump_b(W, s, r, n):
        pump_bh(W, s, r, n, 0)
        pump_bh(W, s, r, n, 1)

    def pump_bw(W, s, r, n):
        pump_bh(W, s, r, n, 2)

    def pump_a1(W, s, r):
        arrived(W.at[pl.ds(0, 2)], r)
        for d in (0, 1):
            w_a2(W, s, r, d).start()

    def pump_a2(W, s, r):
        arrived(W.at[0], r + 1)

    def pump_b1(W, s, r, n):
        arrived(W.at[0], r + 2 + n)
        for d in (0, 1):
            w_b2(W, s, r, n, d).start()

    def pump_bw1(W, s, r, n):
        arrived(W.at[pl.ds(0, 2)], r + 2 + n)
        for d in (0, 1):
            w_b2(W, s, r, n, d).start()

    def pump_b2(W, s, r, n):
        arrived(W.at[0], r + 6 + n)

    def rest_b(W, s, r, n):
        arrived(W.at[0], r + 10 + n)

    U = (UB, 2, 5)
    V = (DB, 3, 57)
    pump_a0(*U)

    ph("d_wait_pa")
    arrived(PB.at[pl.ds(0, 3)], 3)
    for e in (1, 3, 2):
        p_b(e).start()
    pump_bw(*U, 0)
    ph("d_relay")
    arrived(RL, 1)
    for k in (0, 1):
        relay_on(k).start()
    ph("e_Ua1")
    pump_a1(*U)
    pump_bw(*U, 1)
    pump_bw(*U, 2)
    def row_of(ref):
        return jnp.concatenate([ref[pl.ds(2 * t, 1), :], ref[pl.ds(2 * t + 1, 1), :]], axis=1)

    NB[pl.ds(0, 16), :] = jnp.zeros((16, 256), BF16)
    NB[pl.ds(16 + SEQ, 16), :] = jnp.zeros((16, 256), BF16)
    ph("f_wait_x")
    c_x.wait()
    for cp in c_g:
        cp.wait()
    gm = row_of(gmix)
    arrived(R.at[pl.ds(0, 7)], 2)
    arrived(X.at[pl.ds(0, 640)], 0)
    arrived(HX, 20)
    ph("g_normed")
    order = (0, 1, 3, 2)

    def chunk(p, base=0):
        return (y + base + order[p]) % 4

    def rows_at(q):
        return pl.ds(pl.multiple_of(CH * q, CH), CH)

    def norm_tile(i):
        rc = to_column(R[i, 0:1, :])
        xv = X[rows_of(i), :].astype(F32)
        NB[pl.ds(pl.multiple_of(16 + 128 * i, 16), 128), :] = (xv * rc * gm).astype(BF16)

    for p in range(3):
        for h in (0, 1):
            norm_tile(2 * chunk(p) + h)
    for k in (0, 1):
        i = 2 * chunk(3) + k
        rc = to_column(R[i, 0:1, :])[112 * k:112 * k + 16]
        NB[pl.ds(pl.multiple_of(16 + 128 * i + 112 * k, 16), 16), :] = (HX[k].astype(F32) * rc * gm).astype(BF16)

    reach = 1 + (y >= 1).astype(jnp.int32) + 2 * (y >= 2).astype(jnp.int32) + 4 * (y >= 3).astype(jnp.int32)
    bi = lax.broadcasted_iota(jnp.int32, (128, 160), 0)
    bj = lax.broadcasted_iota(jnp.int32, (128, 160), 1)
    delta = bj - 16 - bi
    band = jnp.where((delta >= -reach) & (delta < reach), 1.0, 0.0).astype(BF16)

    def pl_x(p):
        ref = PL2.at[c, rows_at(chunk(p))]
        return remote(ref, ref, 4, 21 + p, f, sib)

    def pool(p):
        for h in (0, 1):
            i = 2 * chunk(p) + h
            sums = jnp.dot(band, NB[pl.ds(pl.multiple_of(128 * i, 128), 160), :], preferred_element_type=F32)
            pos = 128 * i + lax.broadcasted_iota(jnp.int32, (128, 256), 0)
            count = jnp.minimum(pos + reach, SEQ) - jnp.maximum(pos - reach, 0)
            mine = NB[pl.ds(pl.multiple_of(16 + 128 * i, 16), 128), :].astype(F32)
            PL2[c, rows_of(i), :] = (sums / count.astype(F32) - mine).astype(BF16)
        pl_x(p).start()

    ph("h_pool")
    for p in range(3):
        pool(p)

    ph("i_pb")
    arrived(PB.at[pl.ds(0, 12)], 4)
    ph("j_mix")
    psc = row_of(pscale)
    gml = row_of(gmlp)

    def g_ref(owner, q):
        return G.at[owner, rows_at(q)]

    def g_y(p, d):
        ref = g_ref(t, chunk(p))
        return remote(ref, ref, 5, 25 + p, f, yp if d == 0 else ym)

    def g_sib(k, p):
        owner = (t + (0, 6, 2, 4)[k]) % 8
        q = chunk(p, (0, 3, 1, 2)[k])
        ref = g_ref(owner, q)
        return remote(ref, ref, 5, 31 + q, f, sib)

    def g_fwd(p):
        ref = g_ref(ym if p < 2 else yp, chunk(p, 3 if p < 2 else 1))
        return remote(ref, ref, 5, 29 + p % 2, f, yp if p < 2 else ym)

    pk = [jnp.concatenate([PB[slot_of(8 * k + i)] for i in range(8)], axis=0) for k in (0, 1)]

    def mix(p):
        q = chunk(p)
        rows = rows_at(q)
        arrived(PL2.at[1 - c, rows], 21 + p)
        mixed = (jnp.dot(PL2[0, rows, :], pk[0], preferred_element_type=F32)
                 + jnp.dot(PL2[1, rows, :], pk[1], preferred_element_type=F32)) * psc
        first = (X[rows, :].astype(F32) + mixed).astype(BF16).astype(F32)
        G[t, rows, :] = (first * gml).astype(BF16)
        for d in (0, 1):
            g_y(p, d).start()
        g_sib(0, p).start()
        ACC[0, rows, :] = first[:, :128]
        ACC[1, rows, :] = first[:, 128:]
        sq = jnp.sum(first * first, axis=1, keepdims=True)
        for h in (0, 1):
            SQ[t, pl.ds(2 * q + h, 1), :] = to_lanes(sq[128 * h:128 * h + 128])

    for p in range(3):
        mix(p)
    ph("k_far")
    arrived(X.at[pl.ds(0, 256)], 19)
    for h in (0, 1):
        norm_tile(2 * chunk(3) + h)
    pool(3)
    ph("l_Ub0")
    pump_bw1(*U, 0)
    ph("l_Ua2")
    pump_a2(*U)
    pump_b(*U, 3)
    ph("l_mix3")
    mix(3)
    ph("l_sq")

    def sq_x(e):
        return remote(SQ.at[t], SQ.at[t], 1, 35, f, (t + e) % 8)

    for e in range(1, 8):
        sq_x(e).start()

    def g_pump(p):
        arrived(G.at[0, pl.ds(0, 2 * CH)], 25 + p)
        g_fwd(p).start()
        g_sib(1, p).start()
        g_sib(2, p).start()

    def g_pump2(p):
        arrived(G.at[0, pl.ds(0, 2 * CH)], 29 + p)
        g_sib(3, p).start()
        g_sib(3, p + 2).start()

    ph("m_Ub1")
    pump_bw1(*U, 1)
    ph("m_g0")
    g_pump(0)
    def on(core, *todo):
        @pl.when(c == core)
        def _():
            for fn, args in todo:
                fn(*V, *args)

    ph("m_Ub2")
    pump_bw1(*U, 2)
    pump_a0(*V)
    ph("m_g1")
    g_pump(1)
    ph("m_g2")
    g_pump(2)
    ph("n_Ub3")
    pump_b1(*U, 3)
    on(0, (pump_b, (0,)))
    on(1, (pump_bw, (0,)))
    ph("o_g3")
    g_pump(3)
    ph("o_Va1")
    pump_a1(*V)
    on(0, (pump_bh, (1, 0)))
    on(1, (pump_bw, (1,)), (pump_bw, (2,)))
    ph("o_g20")
    g_pump2(0)
    ph("p_Ub2")
    for n in range(4):
        pump_b2(*U, n)
    rest_b(*U, 3)
    ph("p_g21")
    g_pump2(1)
    ph("p_rt")
    arrived(SQ.at[pl.ds(0, 7)], 35)
    total = SQ[0]
    for i in range(1, 8):
        total = total + SQ[i]
    RT[...] = lax.rsqrt(total / D + EPS)

    def up_rows(q):
        arrived(G.at[pl.ds(0, 4), pl.ds(0, CH)], 31 + q)
        ph(f"t_up{q}")
        rows = pl.ds(CH * q, CH)
        rc = jnp.concatenate([to_column(RT[2 * q + h:2 * q + h + 1, :]) for h in (0, 1)], axis=0)
        lhs = jnp.concatenate([G[i, rows, :] for i in range(8)], axis=1)
        rhs = jnp.concatenate([UB[slot_of(g)] for g in range(16)], axis=1)
        pre = lax.dot_general(lhs, rhs, (((1,), (1,)), ((), ())), preferred_element_type=F32)
        act = jnp.maximum(pre * rc, 0.0)
        H[rows, :] = (act * act).astype(BF16)

    eighth = UR // 2

    def mine(j):
        return pl.ds(pl.multiple_of(HALF * c + UR * j, UR), UR)

    def other(j):
        return pl.ds(pl.multiple_of(HALF * (1 - c) + UR * j, UR), UR)

    qrows = (pl.ds(0, eighth), pl.ds(eighth, eighth))

    def column(k):
        xk = (x + offs[k]) % 4
        return xk, xk // 2

    def c_x2(k, j, d):
        return remote(SS.at[k, j, d], SB.at[k, j, d], 4, 36 + 2 * (J * k + j) + (d != 2), f, sib)

    def y_half(k, j, d):
        return remote(SO.at[k, j, 2, qrows[d]], RH.at[k, j, d], 6, 44 + k + 4 * j, f, yp if d == 0 else ym)

    def y_part(k, j, d, h):
        to = 2 * ((y + 1 + 2 * d) % 4) + column(k)[1]
        rows = pl.ds(pl.multiple_of(HALF * c + UR * j + eighth * h, eighth), eighth)
        return remote(SO.at[k, j, 1 + 2 * d, qrows[h]], RY.at[k, d, rows], 6, 48 + k, f, to)

    def z_x(k, j):
        return remote(SO.at[k, j, 0], RZ.at[k, pl.ds(UR * j, UR)], 4, 52 + k, f, sib)

    def pump(n):
        if n == 0:
            on(0, (pump_b1, (0,)), (pump_bh, (1, 1)), (pump_bh, (2, 0)))
        if n == 1:
            on(0, (pump_b1, (1,)), (pump_bh, (2, 1)), (pump_bh, (3, 0)))
            on(1, (pump_bw1, (0,)), (pump_bw1, (1,)))
        if n == 2:
            on(0, (pump_b1, (2,)), (pump_bh, (3, 1)))
            on(1, (pump_bw1, (2,)), (pump_bw1, (3,)))
        if n == 3:
            on(0, (pump_b1, (3,)))
        if n == 4:
            pump_a2(*V)
            on(1, (pump_bw, (3,)))

    def ready(k):
        on(0, (rest_b, (k,)), (pump_b2, (k,)))
        if k == 3:
            on(1, *((pump_b2, (n,)) for n in range(4)))

    def down(k):
        xk, _ = column(k)
        rhs = jnp.concatenate([DB[slot_of(4 * ((y + d) % 4) + xk)] for d in range(4)], axis=1)
        for j in range(J):
            part = jnp.dot(H[other(j), :], rhs, preferred_element_type=F32)
            for d in (2, 1, 3, 0):
                SS[k, j, d] = part[:, 128 * d:128 * d + 128].astype(BF16)
                c_x2(k, j, d).start()
        for j in range(J):
            PART[(2 * k + j) % 4] = jnp.dot(H[mine(j), :], rhs, preferred_element_type=F32)

    def both(k, j, d, rows):
        return PART[(2 * k + j) % 4, rows, 128 * d:128 * d + 128] + SB[k, j, d, rows].astype(F32)

    def stage1(k, j):
        arrived(SB.at[k, j, 2], 36 + 2 * (J * k + j))
        for d in (0, 1):
            SO[k, j, 2, qrows[d]] = both(k, j, 2, qrows[d]).astype(BF16)
            y_half(k, j, d).start()
        arrived(SB.at[k, j, pl.ds(0, 3)], 37 + 2 * (J * k + j))
        for d in (0, 1):
            b = 1 + 2 * d
            SO[k, j, b, qrows[1 - d]] = both(k, j, b, qrows[1 - d]).astype(BF16)
            y_part(k, j, d, 1 - d).start()

    def stage2(k, j):
        xk, keeper = column(k)
        arrived(RH.at[k, j], 44 + k + 4 * j)
        for d in (0, 1):
            b = 1 + 2 * d
            SO[k, j, b, qrows[d]] = (both(k, j, b, qrows[d]) + RH[k, j, d].astype(F32)).astype(BF16)
            y_part(k, j, d, d).start()

        @pl.when(keeper == c)
        def _():
            ACC[xk % 2, mine(j)] = ACC[xk % 2, mine(j)] + both(k, j, 0, pl.ds(0, UR))

        @pl.when(keeper != c)
        def _():
            SO[k, j, 0] = both(k, j, 0, pl.ds(0, UR)).astype(BF16)
            z_x(k, j).start()

    def stage3(k):
        xk, keeper = column(k)

        @pl.when(keeper == c)
        def _():
            arrived(RZ.at[k], 52 + k)
            rest = pl.ds(pl.multiple_of(HALF * (1 - c), HALF), HALF)
            ACC[xk % 2, rest] = ACC[xk % 2, rest] + RZ[k].astype(F32)
            arrived(RY.at[k], 48 + k)
            ACC[xk % 2] = ACC[xk % 2] + RY[k, 0].astype(F32) + RY[k, 1].astype(F32)

    plan = ("p0 u0 p4 u2 u1 p1 u3 r0 d0 100 101 p2 r1 "
            "d1 110 111 200 201 p3 r2 d2 120 121 210 211 r3 d3 130 131 "
            "220 221 30 230 231 31 32 33")
    for step in plan.split():
        ph("w_" + step)
        a = [int(v) for v in step[1:]]
        if len(a) == 2 and a[1] >= J:
            continue
        {"u": up_rows, "p": pump, "r": ready, "d": down, "1": stage1, "2": stage2, "3": stage3}[step[0]](*a)

    ph("y_sq2")
    for i in range(8):
        rows = pl.ds(128 * i, 128)
        a0, a1 = ACC[0, rows, :], ACC[1, rows, :]
        SQ2[t, pl.ds(i, 1), :] = to_lanes(jnp.sum(a0 * a0 + a1 * a1, axis=1, keepdims=True))

    def t_x(e):
        return remote(SQ2.at[t], SQ2.at[t], 1, 56, f, (t + e) % 8)

    for e in range(1, 8):
        t_x(e).start()
    ph("y_wait")
    arrived(SQ2.at[pl.ds(0, 7)], 56)
    total = SQ2[0]
    for i in range(1, 8):
        total = total + SQ2[i]
    rl = lax.rsqrt(total / D + EPS)

    def out_x(q):
        rows = pl.ds(CH * q, CH)
        return pltpu.make_async_copy(X.at[rows], out.at[rows], lsem.at[q])

    for i in range(8):
        rows = pl.ds(128 * i, 128)
        rc = to_column(rl[i:i + 1, :])
        for h in (0, 1):
            X[rows, 128 * h:128 * h + 128] = (ACC[h, rows, :] * rc * gout[h:h + 1, :]).astype(BF16)
        if i % 2 == 1:
            out_x(i // 2).start()

    ph("z_sent")
    relay_out().wait_send()
    for k in (0, 1):
        relay_on(k).wait_send()
        edge(k).wait_send()
    for n in range(5):
        near(n).wait_send()
    for e in range(1, 8):
        r_x(e).wait_send()
        sq_x(e).wait_send()
        t_x(e).wait_send()
    for e in (1, 2, 3):
        p_a(e).wait_send()
        p_b(e).wait_send()
    for W in (U, V):
        for d in (0, 1):
            w_a0(*W, d).wait_send()
            w_a2(*W, d).wait_send()
            for n in range(4):
                w_b(*W, n, d, 2).wait_send()
                w_b2(*W, n, d).wait_send()
    for q in range(NCH):
        pl_x(q).wait_send()
        g_y(q, 0).wait_send()
        g_y(q, 1).wait_send()
        g_fwd(q).wait_send()
        for k in range(4):
            g_sib(k, q).wait_send()
    for k in range(4):
        for j in range(J):
            for d in range(4):
                c_x2(k, j, d).wait_send()
            for d in (0, 1):
                y_half(k, j, d).wait_send()
                y_part(k, j, d, 0).wait_send()
                y_part(k, j, d, 1).wait_send()

        @pl.when(column(k)[1] != c)
        def _():
            for j in range(J):
                z_x(k, j).wait_send()

    for q in range(NCH):
        out_x(q).wait()
    ph(None)


def local(tokens, pool_weight, pool_scale, gain_mix, gain_mlp, w_up, w_down, gain_out):
    dma = pltpu.SemaphoreType.DMA
    hbm = pl.BlockSpec(memory_space=pltpu.HBM)
    return pl.pallas_call(
        kernel,
        out_shape=jax.ShapeDtypeStruct((SEQ, 256), BF16),
        in_specs=[hbm] * 8,
        out_specs=hbm,
        scratch_shapes=[
            pltpu.VMEM((128, D), BF16),
            pltpu.VMEM((128, 512), BF16),
            pltpu.VMEM((2, 16, 256), BF16),
            pltpu.VMEM((SEQ, 256), BF16),
            pltpu.VMEM((SEQ + 32, 256), BF16),
            pltpu.VMEM((8, 8, 128), F32),
            pltpu.VMEM((8, 128), F32),
            pltpu.VMEM((16, 32, 256), BF16),
            pltpu.VMEM((16, 1024, 128), BF16),
            pltpu.VMEM((16, 1024, 128), BF16),
            pltpu.VMEM((2, SEQ, 256), BF16),
            pltpu.VMEM((8, SEQ, 256), BF16),
            pltpu.VMEM((8, 8, 128), F32),
            pltpu.VMEM((8, 8, 128), F32),
            pltpu.VMEM((SEQ, 1024), BF16),
            pltpu.VMEM((4, UR, 512), F32),
            pltpu.VMEM((4, J, 4, UR, 128), BF16),
            pltpu.VMEM((4, J, 4, UR, 128), BF16),
            pltpu.VMEM((4, J, 4, UR, 128), BF16),
            pltpu.VMEM((4, J, 2, UR // 2, 128), BF16),
            pltpu.VMEM((4, 2, SEQ, 128), BF16),
            pltpu.VMEM((4, HALF, 128), BF16),
            pltpu.VMEM((2, SEQ, 128), F32),
            pltpu.VMEM((16, 128), F32),
            pltpu.VMEM((16, 128), F32),
            pltpu.VMEM((16, 128), F32),
            pltpu.VMEM((2, 128), F32),
            dma((9,)),
            dma((7,)),
            dma((71,)),
        ],
        compiler_params=pltpu.CompilerParams(
            collective_id=0, has_side_effects=True, vmem_limit_bytes=60 * 1024 * 1024),
        name="mixers",
    )(tokens, pool_weight, w_up, w_down, pool_scale.reshape(16, 128), gain_mix.reshape(16, 128),
      gain_mlp.reshape(16, 128), gain_out.reshape(2, 128))


def solution(mesh):
    placed = (P(("fs", "tp"), None), P(None, "fs", None), P(), P(), P(), P("tp", "fs"), P("tp", "fs"), P("tp"))
    return jax.shard_map(local, mesh=mesh, in_specs=placed, out_specs=P("fs", "tp"), check_vma=False)
```

```python
import functools

import jax
import jax.numpy as jnp
from jax import lax
from jax.experimental import pallas as pl
from jax.experimental.pallas import tpu as pltpu
from jax.sharding import PartitionSpec as P

D = 2048
SEQ = 1024
EPS = 1e-06
F32 = jnp.float32
BF16 = jnp.bfloat16
MESH = pl.DeviceIdType.MESH
CH = 256
NCH = SEQ // CH
HALF = SEQ // 2
J = 1
UR = HALF // J


class Phases:
    now = None

    def __call__(self, name):
        if self.now is not None:
            self.now.__exit__(None, None, None)
        self.now = jax.named_scope(name) if name else None
        if name:
            self.now.__enter__()


def kernel(tok, pw, up, dn, pscale_h, gmix_h, gmlp_h, gout_h, out,
           tokv, RL, HX, X, NB, R, RT, PB, UB, DB, PL2, G, SQ, SQ2, H, PART, SS, SB, SO, RH, RY, RZ, ACC,
           pscale, gmix, gmlp, gout, lsem, snd, rcv):
    ph = Phases()
    f = lax.axis_index("fs")
    t = lax.axis_index("tp")
    z, x = f // 4, f % 4
    y, c = t // 2, t % 2

    def fa(d):
        return (1 - c) * (4 * z + (x + d) % 4) + c * (4 * ((z + d) % 4) + x)

    def fb(d):
        return (1 - c) * (4 * ((z + d) % 4) + x) + c * (4 * z + (x + d) % 4)

    pa = (1 - c) * x + c * z
    pb = (1 - c) * z + c * x

    def slot(i, j):
        return 4 * ((pb + j) % 4) + (pa + i) % 4

    def slot_of(g):
        return (1 - c) * g + c * (4 * (g % 4) + g // 4)

    def remote(src, dst, ssem, rsem, fs, tp):
        return pltpu.make_async_remote_copy(
            src_ref=src, dst_ref=dst, send_sem=snd.at[ssem], recv_sem=rcv.at[rsem],
            device_id={"fs": fs, "tp": tp}, device_id_type=MESH)

    def arrived(ref, rsem):
        pltpu.make_async_copy(ref, ref, rcv.at[rsem]).wait()

    sib = 2 * y + 1 - c
    yp = 2 * ((y + 1) % 4) + c
    ym = 2 * ((y + 3) % 4) + c
    own = slot(0, 0)

    ph("a_entry")
    c_tok = pltpu.make_async_copy(tok, tokv, lsem.at[0])
    c_x = pltpu.make_async_copy(
        tok.at[:, pl.ds(pl.multiple_of(256 * t, 256), 256)],
        X.at[pl.ds(pl.multiple_of(128 * t, 128), 128)], lsem.at[1])
    c_u = pltpu.make_async_copy(up, UB.at[own], lsem.at[2])
    c_d = pltpu.make_async_copy(dn, DB.at[own], lsem.at[3])
    c_p = pltpu.make_async_copy(
        pw.at[y, :, pl.ds(pl.multiple_of(256 * c, 256), 256)], PB.at[own], lsem.at[4])
    c_g = [pltpu.make_async_copy(h, v, lsem.at[5 + i])
           for i, (h, v) in enumerate(((pscale_h, pscale), (gmix_h, gmix), (gmlp_h, gmlp), (gout_h, gout)))]
    for cp in [c_tok, c_p, c_u, c_x, c_d] + c_g:
        cp.start()
    barrier = pltpu.get_barrier_semaphore()
    for e in range(1, 8):
        pl.semaphore_signal(barrier, inc=1, device_id={"fs": f, "tp": (t + e) % 8}, device_id_type=MESH)
    for e in (1, 2, 3):
        pl.semaphore_signal(barrier, inc=1, device_id={"fs": fa(e), "tp": t}, device_id_type=MESH)
        pl.semaphore_signal(barrier, inc=1, device_id={"fs": fb(e), "tp": t}, device_id_type=MESH)

    ri = lax.broadcasted_iota(jnp.int32, (128, 128), 0)
    ci = lax.broadcasted_iota(jnp.int32, (128, 128), 1)
    eye = (ri == ci).astype(F32)

    def to_lanes(col):
        return jnp.sum(col * eye, axis=0, keepdims=True)

    def to_column(lanes):
        return jnp.sum(lanes * eye, axis=1, keepdims=True)

    c_tok.wait()
    v = tokv[...].astype(F32)
    r1 = lax.rsqrt(jnp.sum(v * v, axis=1, keepdims=True) / D + EPS)
    R[t] = jnp.broadcast_to(to_lanes(r1), (8, 128))
    c_p.wait()
    c_u.wait()
    c_d.wait()
    pl.semaphore_wait(barrier, 13)

    ph("b_start")
    via = (y + 1 + 2 * c) % 4

    def rows_of(o):
        return pl.ds(pl.multiple_of(128 * o, 128), 128)

    def near(n):
        p = (2 * ((y + (1 if n < 2 else 3)) % 4) + n % 2) if n < 4 else sib
        return remote(tokv.at[:, pl.ds(pl.multiple_of(256 * p, 256), 256)], X.at[rows_of(t)], 0, 0, f, p)

    def relay_out():
        return remote(tokv.at[:, pl.ds(pl.multiple_of(512 * ((y + 2) % 4), 512), 512)], RL, 0, 1, f, 2 * via + c)

    def relay_on(k):
        o = 2 * ((y + 3 + 2 * c) % 4) + c
        return remote(RL.at[:, pl.ds(256 * k, 256)], X.at[rows_of(o)], 0, 19, f, 2 * via + k)

    def edge(k):
        p = 2 * ((y + 2) % 4) + k
        return remote(tokv.at[pl.ds(pl.multiple_of(112 * c, 16), 16), pl.ds(pl.multiple_of(256 * p, 256), 256)],
                      HX.at[c], 0, 20, f, p)

    for k in (0, 1):
        edge(k).start()
    relay_out().start()
    for n in (0, 2, 1, 3, 4):
        near(n).start()

    def r_x(e):
        return remote(R.at[t], R.at[t], 1, 2, f, (t + e) % 8)

    for e in range(1, 8):
        r_x(e).start()

    def p_a(e):
        return remote(PB.at[own], PB.at[own], 1, 3, fa(e), t)

    def p_b(e):
        line = PB.at[pl.ds(4 * pb, 4)]
        return remote(line, line, 1, 4, fb(e), t)

    for e in (1, 3, 2):
        p_a(e).start()

    hrows = (pl.ds(0, HALF), pl.ds(HALF, HALF))
    offs = (0, 3, 1, 2)

    def w_a0(W, s, r, d):
        ref = W.at[own]
        return remote(ref, ref, s, r, fa(1 if d == 0 else 3), t)

    def w_a2(W, s, r, d):
        ref = W.at[slot(3 if d == 0 else 1, 0), hrows[d]]
        return remote(ref, ref, s, r + 1, fa(1 if d == 0 else 3), t)

    def w_b(W, s, r, n, d, h):
        ref = W.at[slot(offs[n], 0)] if h == 2 else W.at[slot(offs[n], 0), hrows[d if h == 0 else 1 - d]]
        return remote(ref, ref, s, r + (10 if h == 1 else 2) + n, fb(1 if d == 0 else 3), t)

    def w_b2(W, s, r, n, d):
        ref = W.at[slot(offs[n], 3 if d == 0 else 1), hrows[d]]
        return remote(ref, ref, s, r + 6 + n, fb(1 if d == 0 else 3), t)

    def pump_a0(W, s, r):
        for d in (0, 1):
            w_a0(W, s, r, d).start()

    def pump_bh(W, s, r, n, h):
        for d in (0, 1):
            w_b(W, s, r, n, d, h).start()

    def pump_b(W, s, r, n):
        pump_bh(W, s, r, n, 0)
        pump_bh(W, s, r, n, 1)

    def pump_bw(W, s, r, n):
        pump_bh(W, s, r, n, 2)

    def pump_a1(W, s, r):
        arrived(W.at[pl.ds(0, 2)], r)
        for d in (0, 1):
            w_a2(W, s, r, d).start()

    def pump_a2(W, s, r):
        arrived(W.at[0], r + 1)

    def pump_b1(W, s, r, n):
        arrived(W.at[0], r + 2 + n)
        for d in (0, 1):
            w_b2(W, s, r, n, d).start()

    def pump_bw1(W, s, r, n):
        arrived(W.at[pl.ds(0, 2)], r + 2 + n)
        for d in (0, 1):
            w_b2(W, s, r, n, d).start()

    def pump_b2(W, s, r, n):
        arrived(W.at[0], r + 6 + n)

    def rest_b(W, s, r, n):
        arrived(W.at[0], r + 10 + n)

    U = (UB, 2, 5)
    V = (DB, 3, 57)
    pump_a0(*U)

    ph("d_wait_pa")
    arrived(PB.at[pl.ds(0, 3)], 3)
    for e in (1, 3, 2):
        p_b(e).start()
    pump_bw(*U, 0)
    ph("d_relay")
    arrived(RL, 1)
    for k in (0, 1):
        relay_on(k).start()
    ph("e_Ua1")
    pump_a1(*U)
    pump_bw(*U, 1)
    pump_bw(*U, 2)
    def row_of(ref):
        return jnp.concatenate([ref[pl.ds(2 * t, 1), :], ref[pl.ds(2 * t + 1, 1), :]], axis=1)

    NB[pl.ds(0, 16), :] = jnp.zeros((16, 256), BF16)
    NB[pl.ds(16 + SEQ, 16), :] = jnp.zeros((16, 256), BF16)
    ph("f_wait_x")
    c_x.wait()
    for cp in c_g:
        cp.wait()
    gm = row_of(gmix)
    arrived(R.at[pl.ds(0, 7)], 2)
    arrived(X.at[pl.ds(0, 640)], 0)
    arrived(HX, 20)
    ph("g_normed")
    order = (0, 1, 3, 2)

    def chunk(p, base=0):
        return (y + base + order[p]) % 4

    def rows_at(q):
        return pl.ds(pl.multiple_of(CH * q, CH), CH)

    def norm_tile(i):
        rc = to_column(R[i, 0:1, :])
        xv = X[rows_of(i), :].astype(F32)
        NB[pl.ds(pl.multiple_of(16 + 128 * i, 16), 128), :] = (xv * rc * gm).astype(BF16)

    for p in range(3):
        for h in (0, 1):
            norm_tile(2 * chunk(p) + h)
    for k in (0, 1):
        i = 2 * chunk(3) + k
        rc = to_column(R[i, 0:1, :])[112 * k:112 * k + 16]
        NB[pl.ds(pl.multiple_of(16 + 128 * i + 112 * k, 16), 16), :] = (HX[k].astype(F32) * rc * gm).astype(BF16)

    reach = 1 + (y >= 1).astype(jnp.int32) + 2 * (y >= 2).astype(jnp.int32) + 4 * (y >= 3).astype(jnp.int32)
    bi = lax.broadcasted_iota(jnp.int32, (128, 160), 0)
    bj = lax.broadcasted_iota(jnp.int32, (128, 160), 1)
    delta = bj - 16 - bi
    band = jnp.where((delta >= -reach) & (delta < reach), 1.0, 0.0).astype(BF16)

    def pl_x(p):
        ref = PL2.at[c, rows_at(chunk(p))]
        return remote(ref, ref, 4, 21 + p, f, sib)

    def pool(p):
        for h in (0, 1):
            i = 2 * chunk(p) + h
            sums = jnp.dot(band, NB[pl.ds(pl.multiple_of(128 * i, 128), 160), :], preferred_element_type=F32)
            pos = 128 * i + lax.broadcasted_iota(jnp.int32, (128, 256), 0)
            count = jnp.minimum(pos + reach, SEQ) - jnp.maximum(pos - reach, 0)
            mine = NB[pl.ds(pl.multiple_of(16 + 128 * i, 16), 128), :].astype(F32)
            PL2[c, rows_of(i), :] = (sums / count.astype(F32) - mine).astype(BF16)
        pl_x(p).start()

    ph("h_pool")
    for p in range(3):
        pool(p)

    ph("i_pb")
    arrived(PB.at[pl.ds(0, 12)], 4)
    ph("j_mix")
    psc = row_of(pscale)
    gml = row_of(gmlp)

    def g_ref(owner, q):
        return G.at[owner, rows_at(q)]

    def g_y(p, d):
        ref = g_ref(t, chunk(p))
        return remote(ref, ref, 5, 25 + p, f, yp if d == 0 else ym)

    def g_sib(k, p):
        owner = (t + (0, 6, 2, 4)[k]) % 8
        q = chunk(p, (0, 3, 1, 2)[k])
        ref = g_ref(owner, q)
        return remote(ref, ref, 5, 31 + q, f, sib)

    def g_fwd(p):
        ref = g_ref(ym if p < 2 else yp, chunk(p, 3 if p < 2 else 1))
        return remote(ref, ref, 5, 29 + p % 2, f, yp if p < 2 else ym)

    pk = [jnp.concatenate([PB[slot_of(8 * k + i)] for i in range(8)], axis=0) for k in (0, 1)]

    def mix(p):
        q = chunk(p)
        rows = rows_at(q)
        arrived(PL2.at[1 - c, rows], 21 + p)
        mixed = (jnp.dot(PL2[0, rows, :], pk[0], preferred_element_type=F32)
                 + jnp.dot(PL2[1, rows, :], pk[1], preferred_element_type=F32)) * psc
        first = (X[rows, :].astype(F32) + mixed).astype(BF16).astype(F32)
        G[t, rows, :] = (first * gml).astype(BF16)
        for d in (0, 1):
            g_y(p, d).start()
        g_sib(0, p).start()
        ACC[0, rows, :] = first[:, :128]
        ACC[1, rows, :] = first[:, 128:]
        sq = jnp.sum(first * first, axis=1, keepdims=True)
        for h in (0, 1):
            SQ[t, pl.ds(2 * q + h, 1), :] = to_lanes(sq[128 * h:128 * h + 128])

    for p in range(3):
        mix(p)
    ph("k_far")
    arrived(X.at[pl.ds(0, 256)], 19)
    for h in (0, 1):
        norm_tile(2 * chunk(3) + h)
    pool(3)
    ph("l_Ub0")
    pump_bw1(*U, 0)
    ph("l_Ua2")
    pump_a2(*U)
    pump_b(*U, 3)
    ph("l_mix3")
    mix(3)
    ph("l_sq")

    def sq_x(e):
        return remote(SQ.at[t], SQ.at[t], 1, 35, f, (t + e) % 8)

    for e in range(1, 8):
        sq_x(e).start()

    def g_pump(p):
        arrived(G.at[0, pl.ds(0, 2 * CH)], 25 + p)
        g_fwd(p).start()
        g_sib(1, p).start()
        g_sib(2, p).start()

    def g_pump2(p):
        arrived(G.at[0, pl.ds(0, 2 * CH)], 29 + p)
        g_sib(3, p).start()
        g_sib(3, p + 2).start()

    ph("m_Ub1")
    pump_bw1(*U, 1)
    ph("m_g0")
    g_pump(0)
    def on(core, *todo):
        @pl.when(c == core)
        def _():
            for fn, args in todo:
                fn(*V, *args)

    ph("m_Ub2")
    pump_bw1(*U, 2)
    pump_a0(*V)
    ph("m_g1")
    g_pump(1)
    ph("m_g2")
    g_pump(2)
    ph("n_Ub3")
    pump_b1(*U, 3)
    on(0, (pump_b, (0,)))
    on(1, (pump_bw, (0,)))
    ph("o_g3")
    g_pump(3)
    ph("o_Va1")
    pump_a1(*V)
    on(0, (pump_bh, (1, 0)))
    on(1, (pump_bw, (1,)), (pump_bw, (2,)))
    ph("o_g20")
    g_pump2(0)
    ph("p_g21")
    g_pump2(1)
    ph("p_Ub2")
    for n in range(4):
        pump_b2(*U, n)
    rest_b(*U, 3)
    ph("p_rt")
    arrived(SQ.at[pl.ds(0, 7)], 35)
    total = SQ[0]
    for i in range(1, 8):
        total = total + SQ[i]
    RT[...] = lax.rsqrt(total / D + EPS)

    def up_rows(q):
        arrived(G.at[pl.ds(0, 4), pl.ds(0, CH)], 31 + q)
        ph(f"t_up{q}")
        rows = pl.ds(CH * q, CH)
        rc = jnp.concatenate([to_column(RT[2 * q + h:2 * q + h + 1, :]) for h in (0, 1)], axis=0)
        lhs = jnp.concatenate([G[i, rows, :] for i in range(8)], axis=1)
        rhs = jnp.concatenate([UB[slot_of(g)] for g in range(16)], axis=1)
        pre = lax.dot_general(lhs, rhs, (((1,), (1,)), ((), ())), preferred_element_type=F32)
        act = jnp.maximum(pre * rc, 0.0)
        H[rows, :] = (act * act).astype(BF16)

    eighth = UR // 2

    def mine(j):
        return pl.ds(pl.multiple_of(HALF * c + UR * j, UR), UR)

    def other(j):
        return pl.ds(pl.multiple_of(HALF * (1 - c) + UR * j, UR), UR)

    qrows = (pl.ds(0, eighth), pl.ds(eighth, eighth))

    def column(k):
        xk = (x + offs[k]) % 4
        return xk, xk // 2

    def c_x2(k, j, d):
        return remote(SS.at[k, j, d], SB.at[k, j, d], 4, 36 + 2 * (J * k + j) + (d != 2), f, sib)

    def y_half(k, j, d):
        return remote(SO.at[k, j, 2, qrows[d]], RH.at[k, j, d], 6, 44 + k + 4 * j, f, yp if d == 0 else ym)

    def y_part(k, j, d, h):
        to = 2 * ((y + 1 + 2 * d) % 4) + column(k)[1]
        rows = pl.ds(pl.multiple_of(HALF * c + UR * j + eighth * h, eighth), eighth)
        return remote(SO.at[k, j, 1 + 2 * d, qrows[h]], RY.at[k, d, rows], 6, 48 + k, f, to)

    def z_x(k, j):
        return remote(SO.at[k, j, 0], RZ.at[k, pl.ds(UR * j, UR)], 4, 52 + k, f, sib)

    def pump(n):
        if n == 0:
            on(0, (pump_b1, (0,)), (pump_bh, (1, 1)), (pump_bh, (2, 0)))
        if n == 1:
            on(0, (pump_b1, (1,)), (pump_bh, (2, 1)), (pump_bh, (3, 0)))
            on(1, (pump_bw1, (0,)), (pump_bw1, (1,)))
        if n == 2:
            on(0, (pump_b1, (2,)), (pump_bh, (3, 1)))
            on(1, (pump_bw1, (2,)), (pump_bw1, (3,)))
        if n == 3:
            on(0, (pump_b1, (3,)))
        if n == 4:
            pump_a2(*V)
            on(1, (pump_bw, (3,)))

    def ready(k):
        on(0, (rest_b, (k,)), (pump_b2, (k,)))
        if k == 3:
            on(1, *((pump_b2, (n,)) for n in range(4)))

    def down(k):
        xk, _ = column(k)
        rhs = jnp.concatenate([DB[slot_of(4 * ((y + d) % 4) + xk)] for d in range(4)], axis=1)
        for j in range(J):
            part = jnp.dot(H[other(j), :], rhs, preferred_element_type=F32)
            for d in (2, 1, 3, 0):
                SS[k, j, d] = part[:, 128 * d:128 * d + 128].astype(BF16)
                c_x2(k, j, d).start()
        for j in range(J):
            PART[(2 * k + j) % 4] = jnp.dot(H[mine(j), :], rhs, preferred_element_type=F32)

    def both(k, j, d, rows):
        return PART[(2 * k + j) % 4, rows, 128 * d:128 * d + 128] + SB[k, j, d, rows].astype(F32)

    def stage1(k, j):
        arrived(SB.at[k, j, 2], 36 + 2 * (J * k + j))
        for d in (0, 1):
            SO[k, j, 2, qrows[d]] = both(k, j, 2, qrows[d]).astype(BF16)
            y_half(k, j, d).start()
        arrived(SB.at[k, j, pl.ds(0, 3)], 37 + 2 * (J * k + j))
        for d in (0, 1):
            b = 1 + 2 * d
            SO[k, j, b, qrows[1 - d]] = both(k, j, b, qrows[1 - d]).astype(BF16)
            y_part(k, j, d, 1 - d).start()

    def stage2(k, j):
        xk, keeper = column(k)
        arrived(RH.at[k, j], 44 + k + 4 * j)
        for d in (0, 1):
            b = 1 + 2 * d
            SO[k, j, b, qrows[d]] = (both(k, j, b, qrows[d]) + RH[k, j, d].astype(F32)).astype(BF16)
            y_part(k, j, d, d).start()

        @pl.when(keeper == c)
        def _():
            ACC[xk % 2, mine(j)] = ACC[xk % 2, mine(j)] + both(k, j, 0, pl.ds(0, UR))

        @pl.when(keeper != c)
        def _():
            SO[k, j, 0] = both(k, j, 0, pl.ds(0, UR)).astype(BF16)
            z_x(k, j).start()

    def stage3(k):
        xk, keeper = column(k)

        @pl.when(keeper == c)
        def _():
            arrived(RZ.at[k], 52 + k)
            rest = pl.ds(pl.multiple_of(HALF * (1 - c), HALF), HALF)
            ACC[xk % 2, rest] = ACC[xk % 2, rest] + RZ[k].astype(F32)
            arrived(RY.at[k], 48 + k)
            ACC[xk % 2] = ACC[xk % 2] + RY[k, 0].astype(F32) + RY[k, 1].astype(F32)

    plan = (
        (pump, 0), (up_rows, 0), (pump, 4), (up_rows, 2), (up_rows, 1), (pump, 1),
        (up_rows, 3), (ready, 0), (down, 0), (stage1, 0, 0), (pump, 2), (ready, 1),
        (down, 1), (stage1, 1, 0), (stage2, 0, 0), (pump, 3), (ready, 2), (down, 2),
        (stage1, 2, 0), (stage2, 1, 0), (ready, 3), (down, 3), (stage1, 3, 0), (stage2, 2, 0),
        (stage3, 0), (stage2, 3, 0), (stage3, 1), (stage3, 2), (stage3, 3),
    )
    for step, *which in plan:
        ph("w_" + step.__name__ + str(which[0]))
        step(*which)

    ph("y_sq2")
    for i in range(8):
        rows = pl.ds(128 * i, 128)
        a0, a1 = ACC[0, rows, :], ACC[1, rows, :]
        SQ2[t, pl.ds(i, 1), :] = to_lanes(jnp.sum(a0 * a0 + a1 * a1, axis=1, keepdims=True))

    def t_x(e):
        return remote(SQ2.at[t], SQ2.at[t], 1, 56, f, (t + e) % 8)

    for e in range(1, 8):
        t_x(e).start()
    ph("y_wait")
    arrived(SQ2.at[pl.ds(0, 7)], 56)
    total = SQ2[0]
    for i in range(1, 8):
        total = total + SQ2[i]
    rl = lax.rsqrt(total / D + EPS)

    def out_x(q):
        rows = pl.ds(CH * q, CH)
        return pltpu.make_async_copy(X.at[rows], out.at[rows], lsem.at[q])

    for i in range(8):
        rows = pl.ds(128 * i, 128)
        rc = to_column(rl[i:i + 1, :])
        for h in (0, 1):
            X[rows, 128 * h:128 * h + 128] = (ACC[h, rows, :] * rc * gout[h:h + 1, :]).astype(BF16)
        if i % 2 == 1:
            out_x(i // 2).start()

    ph("z_sent")
    relay_out().wait_send()
    for k in (0, 1):
        relay_on(k).wait_send()
        edge(k).wait_send()
    for n in range(5):
        near(n).wait_send()
    for e in range(1, 8):
        r_x(e).wait_send()
        sq_x(e).wait_send()
        t_x(e).wait_send()
    for e in (1, 2, 3):
        p_a(e).wait_send()
        p_b(e).wait_send()
    for W in (U, V):
        for d in (0, 1):
            w_a0(*W, d).wait_send()
            w_a2(*W, d).wait_send()
            for n in range(4):
                w_b(*W, n, d, 2).wait_send()
                w_b2(*W, n, d).wait_send()
    for q in range(NCH):
        pl_x(q).wait_send()
        g_y(q, 0).wait_send()
        g_y(q, 1).wait_send()
        g_fwd(q).wait_send()
        for k in range(4):
            g_sib(k, q).wait_send()
    for k in range(4):
        for j in range(J):
            for d in range(4):
                c_x2(k, j, d).wait_send()
            for d in (0, 1):
                y_half(k, j, d).wait_send()
                y_part(k, j, d, 0).wait_send()
                y_part(k, j, d, 1).wait_send()

        @pl.when(column(k)[1] != c)
        def _():
            for j in range(J):
                z_x(k, j).wait_send()

    for q in range(NCH):
        out_x(q).wait()
    ph(None)


def local(tokens, pool_weight, pool_scale, gain_mix, gain_mlp, w_up, w_down, gain_out):
    dma = pltpu.SemaphoreType.DMA
    hbm = pl.BlockSpec(memory_space=pltpu.HBM)
    return pl.pallas_call(
        kernel,
        out_shape=jax.ShapeDtypeStruct((SEQ, 256), BF16),
        in_specs=[hbm] * 8,
        out_specs=hbm,
        scratch_shapes=[
            pltpu.VMEM((128, D), BF16),
            pltpu.VMEM((128, 512), BF16),
            pltpu.VMEM((2, 16, 256), BF16),
            pltpu.VMEM((SEQ, 256), BF16),
            pltpu.VMEM((SEQ + 32, 256), BF16),
            pltpu.VMEM((8, 8, 128), F32),
            pltpu.VMEM((8, 128), F32),
            pltpu.VMEM((16, 32, 256), BF16),
            pltpu.VMEM((16, 1024, 128), BF16),
            pltpu.VMEM((16, 1024, 128), BF16),
            pltpu.VMEM((2, SEQ, 256), BF16),
            pltpu.VMEM((8, SEQ, 256), BF16),
            pltpu.VMEM((8, 8, 128), F32),
            pltpu.VMEM((8, 8, 128), F32),
            pltpu.VMEM((SEQ, 1024), BF16),
            pltpu.VMEM((4, UR, 512), F32),
            pltpu.VMEM((4, J, 4, UR, 128), BF16),
            pltpu.VMEM((4, J, 4, UR, 128), BF16),
            pltpu.VMEM((4, J, 4, UR, 128), BF16),
            pltpu.VMEM((4, J, 2, UR // 2, 128), BF16),
            pltpu.VMEM((4, 2, SEQ, 128), BF16),
            pltpu.VMEM((4, HALF, 128), BF16),
            pltpu.VMEM((2, SEQ, 128), F32),
            pltpu.VMEM((16, 128), F32),
            pltpu.VMEM((16, 128), F32),
            pltpu.VMEM((16, 128), F32),
            pltpu.VMEM((2, 128), F32),
            dma((9,)),
            dma((7,)),
            dma((71,)),
        ],
        compiler_params=pltpu.CompilerParams(
            collective_id=0, has_side_effects=True, vmem_limit_bytes=60 * 1024 * 1024),
        name="mixers",
    )(tokens, pool_weight, w_up, w_down, pool_scale.reshape(16, 128), gain_mix.reshape(16, 128),
      gain_mlp.reshape(16, 128), gain_out.reshape(2, 128))


def solution(mesh):
    placed = (P(("fs", "tp"), None), P(None, "fs", None), P(), P(), P(), P("tp", "fs"), P("tp", "fs"), P("tp"))
    return jax.shard_map(local, mesh=mesh, in_specs=placed, out_specs=P("fs", "tp"), check_vma=False)
```

```python
import functools

import jax
import jax.numpy as jnp
from jax import lax
from jax.experimental import pallas as pl
from jax.experimental.pallas import tpu as pltpu
from jax.sharding import PartitionSpec as P

D = 2048
SEQ = 1024
EPS = 1e-06
F32 = jnp.float32
BF16 = jnp.bfloat16
MESH = pl.DeviceIdType.MESH
CH = 256
NCH = SEQ // CH
HALF = SEQ // 2
J = 1
UR = HALF // J


class Phases:
    now = None

    def __call__(self, name):
        if self.now is not None:
            self.now.__exit__(None, None, None)
        self.now = jax.named_scope(name) if name else None
        if name:
            self.now.__enter__()


def kernel(tok, pw, up, dn, pscale_h, gmix_h, gmlp_h, gout_h, out,
           tokv, RL, HX, X, NB, R, RT, PB, UB, DB, PL2, G, SQ, SQ2, H, PART, SS, SB, SO, RH, RY, RZ, ACC,
           pscale, gmix, gmlp, gout, lsem, snd, rcv):
    ph = Phases()
    f = lax.axis_index("fs")
    t = lax.axis_index("tp")
    z, x = f // 4, f % 4
    y, c = t // 2, t % 2

    def fa(d):
        return (1 - c) * (4 * z + (x + d) % 4) + c * (4 * ((z + d) % 4) + x)

    def fb(d):
        return (1 - c) * (4 * ((z + d) % 4) + x) + c * (4 * z + (x + d) % 4)

    pa = (1 - c) * x + c * z
    pb = (1 - c) * z + c * x

    def slot(i, j):
        return 4 * ((pb + j) % 4) + (pa + i) % 4

    def slot_of(g):
        return (1 - c) * g + c * (4 * (g % 4) + g // 4)

    def remote(src, dst, ssem, rsem, fs, tp):
        return pltpu.make_async_remote_copy(
            src_ref=src, dst_ref=dst, send_sem=snd.at[ssem], recv_sem=rcv.at[rsem],
            device_id={"fs": fs, "tp": tp}, device_id_type=MESH)

    def arrived(ref, rsem):
        pltpu.make_async_copy(ref, ref, rcv.at[rsem]).wait()

    sib = 2 * y + 1 - c
    yp = 2 * ((y + 1) % 4) + c
    ym = 2 * ((y + 3) % 4) + c
    own = slot(0, 0)

    ph("a_entry")
    c_tok = pltpu.make_async_copy(tok, tokv, lsem.at[0])
    c_x = pltpu.make_async_copy(
        tok.at[:, pl.ds(pl.multiple_of(256 * t, 256), 256)],
        X.at[pl.ds(pl.multiple_of(128 * t, 128), 128)], lsem.at[1])
    c_u = pltpu.make_async_copy(up, UB.at[own], lsem.at[2])
    c_d = pltpu.make_async_copy(dn, DB.at[own], lsem.at[3])
    c_p = pltpu.make_async_copy(
        pw.at[y, :, pl.ds(pl.multiple_of(256 * c, 256), 256)], PB.at[own], lsem.at[4])
    c_g = [pltpu.make_async_copy(h, v, lsem.at[5 + i])
           for i, (h, v) in enumerate(((pscale_h, pscale), (gmix_h, gmix), (gmlp_h, gmlp), (gout_h, gout)))]
    for cp in [c_tok, c_p, c_u, c_x, c_d] + c_g:
        cp.start()
    barrier = pltpu.get_barrier_semaphore()
    for e in range(1, 8):
        pl.semaphore_signal(barrier, inc=1, device_id={"fs": f, "tp": (t + e) % 8}, device_id_type=MESH)
    for e in (1, 2, 3):
        pl.semaphore_signal(barrier, inc=1, device_id={"fs": fa(e), "tp": t}, device_id_type=MESH)
        pl.semaphore_signal(barrier, inc=1, device_id={"fs": fb(e), "tp": t}, device_id_type=MESH)

    ri = lax.broadcasted_iota(jnp.int32, (128, 128), 0)
    ci = lax.broadcasted_iota(jnp.int32, (128, 128), 1)
    eye = (ri == ci).astype(F32)

    def to_lanes(col):
        return jnp.sum(col * eye, axis=0, keepdims=True)

    def to_column(lanes):
        return jnp.sum(lanes * eye, axis=1, keepdims=True)

    c_tok.wait()
    v = tokv[...].astype(F32)
    r1 = lax.rsqrt(jnp.sum(v * v, axis=1, keepdims=True) / D + EPS)
    R[t] = jnp.broadcast_to(to_lanes(r1), (8, 128))
    c_p.wait()
    c_u.wait()
    c_d.wait()
    pl.semaphore_wait(barrier, 13)

    ph("b_start")
    via = (y + 1 + 2 * c) % 4

    def rows_of(o):
        return pl.ds(pl.multiple_of(128 * o, 128), 128)

    def near(n):
        p = (2 * ((y + (1 if n < 2 else 3)) % 4) + n % 2) if n < 4 else sib
        return remote(tokv.at[:, pl.ds(pl.multiple_of(256 * p, 256), 256)], X.at[rows_of(t)], 0, 0, f, p)

    def relay_out():
        return remote(tokv.at[:, pl.ds(pl.multiple_of(512 * ((y + 2) % 4), 512), 512)], RL, 0, 1, f, 2 * via + c)

    def relay_on(k):
        o = 2 * ((y + 3 + 2 * c) % 4) + c
        return remote(RL.at[:, pl.ds(256 * k, 256)], X.at[rows_of(o)], 0, 19, f, 2 * via + k)

    def edge(k):
        p = 2 * ((y + 2) % 4) + k
        return remote(tokv.at[pl.ds(pl.multiple_of(112 * c, 16), 16), pl.ds(pl.multiple_of(256 * p, 256), 256)],
                      HX.at[c], 0, 20, f, p)

    for k in (0, 1):
        edge(k).start()
    relay_out().start()
    for n in (0, 2, 1, 3, 4):
        near(n).start()

    def r_x(e):
        return remote(R.at[t], R.at[t], 1, 2, f, (t + e) % 8)

    for e in range(1, 8):
        r_x(e).start()

    def p_a(e):
        return remote(PB.at[own], PB.at[own], 1, 3, fa(e), t)

    def p_b(e):
        line = PB.at[pl.ds(4 * pb, 4)]
        return remote(line, line, 1, 4, fb(e), t)

    for e in (1, 3, 2):
        p_a(e).start()

    hrows = (pl.ds(0, HALF), pl.ds(HALF, HALF))
    offs = (0, 3, 1, 2)

    def w_a0(W, s, r, d):
        ref = W.at[own]
        return remote(ref, ref, s, r, fa(1 if d == 0 else 3), t)

    def w_a2(W, s, r, d):
        ref = W.at[slot(3 if d == 0 else 1, 0), hrows[d]]
        return remote(ref, ref, s, r + 1, fa(1 if d == 0 else 3), t)

    def w_b(W, s, r, n, d, h):
        ref = W.at[slot(offs[n], 0)] if h == 2 else W.at[slot(offs[n], 0), hrows[d if h == 0 else 1 - d]]
        return remote(ref, ref, s, r + (10 if h == 1 else 2) + n, fb(1 if d == 0 else 3), t)

    def w_b2(W, s, r, n, d):
        ref = W.at[slot(offs[n], 3 if d == 0 else 1), hrows[d]]
        return remote(ref, ref, s, r + 6 + n, fb(1 if d == 0 else 3), t)

    def pump_a0(W, s, r):
        for d in (0, 1):
            w_a0(W, s, r, d).start()

    def pump_bh(W, s, r, n, h):
        for d in (0, 1):
            w_b(W, s, r, n, d, h).start()

    def pump_b(W, s, r, n):
        pump_bh(W, s, r, n, 0)
        pump_bh(W, s, r, n, 1)

    def pump_bw(W, s, r, n):
        pump_bh(W, s, r, n, 2)

    def pump_a1(W, s, r):
        arrived(W.at[pl.ds(0, 2)], r)
        for d in (0, 1):
            w_a2(W, s, r, d).start()

    def pump_a2(W, s, r):
        arrived(W.at[0], r + 1)

    def pump_b1(W, s, r, n):
        arrived(W.at[0], r + 2 + n)
        for d in (0, 1):
            w_b2(W, s, r, n, d).start()

    def pump_bw1(W, s, r, n):
        arrived(W.at[pl.ds(0, 2)], r + 2 + n)
        for d in (0, 1):
            w_b2(W, s, r, n, d).start()

    def pump_b2(W, s, r, n):
        arrived(W.at[0], r + 6 + n)

    def rest_b(W, s, r, n):
        arrived(W.at[0], r + 10 + n)

    U = (UB, 2, 5)
    V = (DB, 3, 57)
    pump_a0(*U)

    ph("d_wait_pa")
    arrived(PB.at[pl.ds(0, 3)], 3)
    for e in (1, 3, 2):
        p_b(e).start()
    pump_bw(*U, 0)
    ph("d_relay")
    arrived(RL, 1)
    for k in (0, 1):
        relay_on(k).start()
    ph("e_Ua1")
    pump_a1(*U)
    pump_bw(*U, 1)
    pump_bw(*U, 2)
    def row_of(ref):
        return jnp.concatenate([ref[pl.ds(2 * t, 1), :], ref[pl.ds(2 * t + 1, 1), :]], axis=1)

    NB[pl.ds(0, 16), :] = jnp.zeros((16, 256), BF16)
    NB[pl.ds(16 + SEQ, 16), :] = jnp.zeros((16, 256), BF16)
    ph("f_wait_x")
    c_x.wait()
    for cp in c_g:
        cp.wait()
    gm = row_of(gmix)
    arrived(R.at[pl.ds(0, 7)], 2)
    arrived(X.at[pl.ds(0, 640)], 0)
    arrived(HX, 20)
    ph("g_normed")
    order = (0, 1, 3, 2)

    def chunk(p, base=0):
        return (y + base + order[p]) % 4

    def rows_at(q):
        return pl.ds(pl.multiple_of(CH * q, CH), CH)

    def norm_tile(i):
        rc = to_column(R[i, 0:1, :])
        xv = X[rows_of(i), :].astype(F32)
        NB[pl.ds(pl.multiple_of(16 + 128 * i, 16), 128), :] = (xv * rc * gm).astype(BF16)

    for p in range(3):
        for h in (0, 1):
            norm_tile(2 * chunk(p) + h)
    for k in (0, 1):
        i = 2 * chunk(3) + k
        rc = to_column(R[i, 0:1, :])[112 * k:112 * k + 16]
        NB[pl.ds(pl.multiple_of(16 + 128 * i + 112 * k, 16), 16), :] = (HX[k].astype(F32) * rc * gm).astype(BF16)

    reach = 1 + (y >= 1).astype(jnp.int32) + 2 * (y >= 2).astype(jnp.int32) + 4 * (y >= 3).astype(jnp.int32)
    bi = lax.broadcasted_iota(jnp.int32, (128, 160), 0)
    bj = lax.broadcasted_iota(jnp.int32, (128, 160), 1)
    delta = bj - 16 - bi
    band = jnp.where((delta >= -reach) & (delta < reach), 1.0, 0.0).astype(BF16)

    def pl_x(p):
        ref = PL2.at[c, rows_at(chunk(p))]
        return remote(ref, ref, 4, 21 + p, f, sib)

    def pool(p):
        for h in (0, 1):
            i = 2 * chunk(p) + h
            sums = jnp.dot(band, NB[pl.ds(pl.multiple_of(128 * i, 128), 160), :], preferred_element_type=F32)
            pos = 128 * i + lax.broadcasted_iota(jnp.int32, (128, 256), 0)
            count = jnp.minimum(pos + reach, SEQ) - jnp.maximum(pos - reach, 0)
            mine = NB[pl.ds(pl.multiple_of(16 + 128 * i, 16), 128), :].astype(F32)
            PL2[c, rows_of(i), :] = (sums / count.astype(F32) - mine).astype(BF16)
        pl_x(p).start()

    ph("h_pool")
    for p in range(3):
        pool(p)

    ph("i_pb")
    arrived(PB.at[pl.ds(0, 12)], 4)
    ph("j_mix")
    psc = row_of(pscale)
    gml = row_of(gmlp)

    def g_ref(owner, q):
        return G.at[owner, rows_at(q)]

    def g_y(p, d):
        ref = g_ref(t, chunk(p))
        return remote(ref, ref, 5, 25 + p, f, yp if d == 0 else ym)

    def g_sib(k, p):
        owner = (t + (0, 6, 2, 4)[k]) % 8
        q = chunk(p, (0, 3, 1, 2)[k])
        ref = g_ref(owner, q)
        return remote(ref, ref, 5, 31 + q, f, sib)

    def g_fwd(p):
        ref = g_ref(ym if p < 2 else yp, chunk(p, 3 if p < 2 else 1))
        return remote(ref, ref, 5, 29 + p % 2, f, yp if p < 2 else ym)

    pk = [jnp.concatenate([PB[slot_of(8 * k + i)] for i in range(8)], axis=0) for k in (0, 1)]

    def mix(p):
        q = chunk(p)
        rows = rows_at(q)
        arrived(PL2.at[1 - c, rows], 21 + p)
        mixed = (jnp.dot(PL2[0, rows, :], pk[0], preferred_element_type=F32)
                 + jnp.dot(PL2[1, rows, :], pk[1], preferred_element_type=F32)) * psc
        first = (X[rows, :].astype(F32) + mixed).astype(BF16).astype(F32)
        G[t, rows, :] = (first * gml).astype(BF16)
        for d in (0, 1):
            g_y(p, d).start()
        g_sib(0, p).start()
        ACC[0, rows, :] = first[:, :128]
        ACC[1, rows, :] = first[:, 128:]
        sq = jnp.sum(first * first, axis=1, keepdims=True)
        for h in (0, 1):
            SQ[t, pl.ds(2 * q + h, 1), :] = to_lanes(sq[128 * h:128 * h + 128])

    for p in range(3):
        mix(p)
    ph("k_far")
    arrived(X.at[pl.ds(0, 256)], 19)
    for h in (0, 1):
        norm_tile(2 * chunk(3) + h)
    pool(3)
    ph("l_Ub0")
    pump_bw1(*U, 0)
    ph("l_Ua2")
    pump_a2(*U)
    pump_b(*U, 3)
    ph("l_mix3")
    mix(3)
    ph("l_sq")

    def sq_x(e):
        return remote(SQ.at[t], SQ.at[t], 1, 35, f, (t + e) % 8)

    for e in range(1, 8):
        sq_x(e).start()

    def g_pump(p):
        arrived(G.at[0, pl.ds(0, 2 * CH)], 25 + p)
        g_fwd(p).start()
        g_sib(1, p).start()
        g_sib(2, p).start()

    def g_pump2(p):
        arrived(G.at[0, pl.ds(0, 2 * CH)], 29 + p)
        g_sib(3, p).start()
        g_sib(3, p + 2).start()

    ph("m_Ub1")
    pump_bw1(*U, 1)
    ph("m_g0")
    g_pump(0)
    def on(core, *todo):
        @pl.when(c == core)
        def _():
            for fn, args in todo:
                fn(*V, *args)

    ph("m_Ub2")
    pump_bw1(*U, 2)
    pump_a0(*V)
    ph("m_g1")
    g_pump(1)
    ph("m_g2")
    g_pump(2)
    ph("n_Ub3")
    pump_b1(*U, 3)
    on(0, (pump_b, (0,)))
    on(1, (pump_bw, (0,)))
    ph("o_g3")
    g_pump(3)
    ph("o_Va1")
    pump_a1(*V)
    on(0, (pump_bh, (1, 0)))
    on(1, (pump_bw, (1,)), (pump_bw, (2,)))
    ph("o_g20")
    g_pump2(0)
    ph("p_g21")
    g_pump2(1)
    ph("p_Ub2")
    for n in range(4):
        pump_b2(*U, n)
    rest_b(*U, 3)
    ph("p_rt")
    arrived(SQ.at[pl.ds(0, 7)], 35)
    total = SQ[0]
    for i in range(1, 8):
        total = total + SQ[i]
    RT[...] = lax.rsqrt(total / D + EPS)

    def up_rows(q):
        arrived(G.at[pl.ds(0, 4), pl.ds(0, CH)], 31 + q)
        ph(f"t_up{q}")
        rows = pl.ds(CH * q, CH)
        rc = jnp.concatenate([to_column(RT[2 * q + h:2 * q + h + 1, :]) for h in (0, 1)], axis=0)
        lhs = jnp.concatenate([G[i, rows, :] for i in range(8)], axis=1)
        rhs = jnp.concatenate([UB[slot_of(g)] for g in range(16)], axis=1)
        pre = lax.dot_general(lhs, rhs, (((1,), (1,)), ((), ())), preferred_element_type=F32)
        act = jnp.maximum(pre * rc, 0.0)
        H[rows, :] = (act * act).astype(BF16)

    eighth = UR // 2

    def mine(j):
        return pl.ds(pl.multiple_of(HALF * c + UR * j, UR), UR)

    def other(j):
        return pl.ds(pl.multiple_of(HALF * (1 - c) + UR * j, UR), UR)

    qrows = (pl.ds(0, eighth), pl.ds(eighth, eighth))

    def column(k):
        xk = (x + offs[k]) % 4
        return xk, xk // 2

    def c_x2(k, j, d):
        return remote(SS.at[k, j, d], SB.at[k, j, d], 4, 36 + 2 * (J * k + j) + (d != 2), f, sib)

    def y_half(k, j, d):
        return remote(SO.at[k, j, 2, qrows[d]], RH.at[k, j, d], 6, 44 + k + 4 * j, f, yp if d == 0 else ym)

    def y_part(k, j, d, h):
        to = 2 * ((y + 1 + 2 * d) % 4) + column(k)[1]
        rows = pl.ds(pl.multiple_of(HALF * c + UR * j + eighth * h, eighth), eighth)
        return remote(SO.at[k, j, 1 + 2 * d, qrows[h]], RY.at[k, d, rows], 6, 48 + k, f, to)

    def z_x(k, j):
        return remote(SO.at[k, j, 0], RZ.at[k, pl.ds(UR * j, UR)], 4, 52 + k, f, sib)

    def pump(n):
        if n == 0:
            on(0, (pump_b1, (0,)), (pump_bh, (1, 1)), (pump_bh, (2, 0)))
        if n == 1:
            on(0, (pump_b1, (1,)), (pump_bh, (2, 1)), (pump_bh, (3, 0)))
            on(1, (pump_bw1, (0,)), (pump_bw1, (1,)))
        if n == 2:
            on(0, (pump_b1, (2,)), (pump_bh, (3, 1)))
            on(1, (pump_bw1, (2,)), (pump_bw1, (3,)))
        if n == 3:
            on(0, (pump_b1, (3,)))
        if n == 4:
            pump_a2(*V)
            on(1, (pump_bw, (3,)))

    def ready(k):
        on(0, (rest_b, (k,)), (pump_b2, (k,)))
        if k == 3:
            on(1, *((pump_b2, (n,)) for n in range(4)))

    def down(k):
        xk, _ = column(k)
        rhs = jnp.concatenate([DB[slot_of(4 * ((y + d) % 4) + xk)] for d in range(4)], axis=1)
        for j in range(J):
            part = jnp.dot(H[other(j), :], rhs, preferred_element_type=F32)
            for d in (2, 1, 3, 0):
                SS[k, j, d] = part[:, 128 * d:128 * d + 128].astype(BF16)
                c_x2(k, j, d).start()
        for j in range(J):
            PART[(2 * k + j) % 4] = jnp.dot(H[mine(j), :], rhs, preferred_element_type=F32)

    def both(k, j, d, rows):
        return PART[(2 * k + j) % 4, rows, 128 * d:128 * d + 128] + SB[k, j, d, rows].astype(F32)

    def stage1(k, j):
        arrived(SB.at[k, j, 2], 36 + 2 * (J * k + j))
        for d in (0, 1):
            SO[k, j, 2, qrows[d]] = both(k, j, 2, qrows[d]).astype(BF16)
            y_half(k, j, d).start()
        arrived(SB.at[k, j, pl.ds(0, 3)], 37 + 2 * (J * k + j))
        for d in (0, 1):
            b = 1 + 2 * d
            SO[k, j, b, qrows[1 - d]] = both(k, j, b, qrows[1 - d]).astype(BF16)
            y_part(k, j, d, 1 - d).start()

    def stage2(k, j):
        xk, keeper = column(k)
        arrived(RH.at[k, j], 44 + k + 4 * j)
        for d in (0, 1):
            b = 1 + 2 * d
            SO[k, j, b, qrows[d]] = (both(k, j, b, qrows[d]) + RH[k, j, d].astype(F32)).astype(BF16)
            y_part(k, j, d, d).start()

        @pl.when(keeper == c)
        def _():
            ACC[xk % 2, mine(j)] = ACC[xk % 2, mine(j)] + both(k, j, 0, pl.ds(0, UR))

        @pl.when(keeper != c)
        def _():
            SO[k, j, 0] = both(k, j, 0, pl.ds(0, UR)).astype(BF16)
            z_x(k, j).start()

    def stage3(k):
        xk, keeper = column(k)

        @pl.when(keeper == c)
        def _():
            arrived(RZ.at[k], 52 + k)
            rest = pl.ds(pl.multiple_of(HALF * (1 - c), HALF), HALF)
            ACC[xk % 2, rest] = ACC[xk % 2, rest] + RZ[k].astype(F32)
            arrived(RY.at[k], 48 + k)
            ACC[xk % 2] = ACC[xk % 2] + RY[k, 0].astype(F32) + RY[k, 1].astype(F32)

    plan = (
        (pump, 0), (up_rows, 0), (pump, 4), (up_rows, 2), (up_rows, 1), (pump, 1),
        (up_rows, 3), (ready, 0), (down, 0), (stage1, 0, 0), (pump, 2), (ready, 1),
        (down, 1), (stage1, 1, 0), (stage2, 0, 0), (pump, 3), (ready, 2), (down, 2),
        (stage1, 2, 0), (stage2, 1, 0), (ready, 3), (down, 3), (stage1, 3, 0), (stage2, 2, 0),
        (stage3, 0), (stage2, 3, 0), (stage3, 1), (stage3, 2), (stage3, 3),
    )
    last = column(3)[0] % 2

    def squares(half):
        return [to_lanes(jnp.sum(ACC[half, pl.ds(128 * i, 128), :] * ACC[half, pl.ds(128 * i, 128), :],
                                 axis=1, keepdims=True)) for i in range(8)]

    for step, *which in plan:
        if step is stage3 and which[0] == 3:
            SQ2[t] = jnp.concatenate(squares(1 - last), axis=0)
        ph("w_" + step.__name__ + str(which[0]))
        step(*which)

    ph("y_sq2")
    SQ2[t] = SQ2[t] + jnp.concatenate(squares(last), axis=0)

    def t_x(e):
        return remote(SQ2.at[t], SQ2.at[t], 1, 56, f, (t + e) % 8)

    for e in range(1, 8):
        t_x(e).start()
    ph("y_wait")
    arrived(SQ2.at[pl.ds(0, 7)], 56)
    total = SQ2[0]
    for i in range(1, 8):
        total = total + SQ2[i]
    rl = lax.rsqrt(total / D + EPS)

    def out_x(q):
        rows = pl.ds(CH * q, CH)
        return pltpu.make_async_copy(X.at[rows], out.at[rows], lsem.at[q])

    for i in range(8):
        rows = pl.ds(128 * i, 128)
        rc = to_column(rl[i:i + 1, :])
        for h in (0, 1):
            X[rows, 128 * h:128 * h + 128] = (ACC[h, rows, :] * rc * gout[h:h + 1, :]).astype(BF16)
        if i % 2 == 1:
            out_x(i // 2).start()

    ph("z_sent")
    relay_out().wait_send()
    for k in (0, 1):
        relay_on(k).wait_send()
        edge(k).wait_send()
    for n in range(5):
        near(n).wait_send()
    for e in range(1, 8):
        r_x(e).wait_send()
        sq_x(e).wait_send()
        t_x(e).wait_send()
    for e in (1, 2, 3):
        p_a(e).wait_send()
        p_b(e).wait_send()
    for W in (U, V):
        for d in (0, 1):
            w_a0(*W, d).wait_send()
            w_a2(*W, d).wait_send()
            for n in range(4):
                w_b(*W, n, d, 2).wait_send()
                w_b2(*W, n, d).wait_send()
    for q in range(NCH):
        pl_x(q).wait_send()
        g_y(q, 0).wait_send()
        g_y(q, 1).wait_send()
        g_fwd(q).wait_send()
        for k in range(4):
            g_sib(k, q).wait_send()
    for k in range(4):
        for j in range(J):
            for d in range(4):
                c_x2(k, j, d).wait_send()
            for d in (0, 1):
                y_half(k, j, d).wait_send()
                y_part(k, j, d, 0).wait_send()
                y_part(k, j, d, 1).wait_send()

        @pl.when(column(k)[1] != c)
        def _():
            for j in range(J):
                z_x(k, j).wait_send()

    for q in range(NCH):
        out_x(q).wait()
    ph(None)


def local(tokens, pool_weight, pool_scale, gain_mix, gain_mlp, w_up, w_down, gain_out):
    dma = pltpu.SemaphoreType.DMA
    hbm = pl.BlockSpec(memory_space=pltpu.HBM)
    return pl.pallas_call(
        kernel,
        out_shape=jax.ShapeDtypeStruct((SEQ, 256), BF16),
        in_specs=[hbm] * 8,
        out_specs=hbm,
        scratch_shapes=[
            pltpu.VMEM((128, D), BF16),
            pltpu.VMEM((128, 512), BF16),
            pltpu.VMEM((2, 16, 256), BF16),
            pltpu.VMEM((SEQ, 256), BF16),
            pltpu.VMEM((SEQ + 32, 256), BF16),
            pltpu.VMEM((8, 8, 128), F32),
            pltpu.VMEM((8, 128), F32),
            pltpu.VMEM((16, 32, 256), BF16),
            pltpu.VMEM((16, 1024, 128), BF16),
            pltpu.VMEM((16, 1024, 128), BF16),
            pltpu.VMEM((2, SEQ, 256), BF16),
            pltpu.VMEM((8, SEQ, 256), BF16),
            pltpu.VMEM((8, 8, 128), F32),
            pltpu.VMEM((8, 8, 128), F32),
            pltpu.VMEM((SEQ, 1024), BF16),
            pltpu.VMEM((4, UR, 512), F32),
            pltpu.VMEM((4, J, 4, UR, 128), BF16),
            pltpu.VMEM((4, J, 4, UR, 128), BF16),
            pltpu.VMEM((4, J, 4, UR, 128), BF16),
            pltpu.VMEM((4, J, 2, UR // 2, 128), BF16),
            pltpu.VMEM((4, 2, SEQ, 128), BF16),
            pltpu.VMEM((4, HALF, 128), BF16),
            pltpu.VMEM((2, SEQ, 128), F32),
            pltpu.VMEM((16, 128), F32),
            pltpu.VMEM((16, 128), F32),
            pltpu.VMEM((16, 128), F32),
            pltpu.VMEM((2, 128), F32),
            dma((9,)),
            dma((7,)),
            dma((71,)),
        ],
        compiler_params=pltpu.CompilerParams(
            collective_id=0, has_side_effects=True, vmem_limit_bytes=60 * 1024 * 1024),
        name="mixers",
    )(tokens, pool_weight, w_up, w_down, pool_scale.reshape(16, 128), gain_mix.reshape(16, 128),
      gain_mlp.reshape(16, 128), gain_out.reshape(2, 128))


def solution(mesh):
    placed = (P(("fs", "tp"), None), P(None, "fs", None), P(), P(), P(), P("tp", "fs"), P("tp", "fs"), P("tp"))
    return jax.shard_map(local, mesh=mesh, in_specs=placed, out_specs=P("fs", "tp"), check_vma=False)
```
